256 devices in a mesh: sp: 64 (over z, y, core), tp: 4 (over x).
Axes of the slice: x: 4, y: 4, z: 8, core: 2. Of those that a mesh axis runs over, the one named last changes fastest.
Arguments:
- tokens: bfloat16 [24576, 2048], P('sp', 'tp'), may hold values from -6 to 6
- norm_gain: float32 [3, 2048], replicated, may hold values from 0.1 to 1.9
- w_value: bfloat16 [3, 2048, 1024], P(None, 'sp', 'tp'), may hold values from -0.125 to 0.125
- w_gate: bfloat16 [3, 2048, 1024], P(None, 'sp', 'tp'), may hold values from -0.125 to 0.125
- conv_taps: float32 [3, 31, 1024], P(None, None, 'tp'), may hold values from -2.4 to 2.4
- conv_bias: float32 [3, 1024], P(None, 'tp'), may hold values from -3 to 3
- ln_gain: float32 [3, 1024], P(None, 'tp'), may hold values from 0.1 to 1.9
- ln_shift: float32 [3, 1024], P(None, 'tp'), may hold values from -3 to 3
- w_out: bfloat16 [3, 1024, 2048], P(None, 'tp', 'sp'), may hold values from -0.1875 to 0.1875
Outputs:
- stream: bfloat16 [24576, 2048], P('sp', 'tp')
The draws below stay inside these ranges and needn't reach their ends.
All inputs are finite; a program needn't handle non-finite values.
Results may differ from the reference program's by a relative error of at most 0.015.
Values may be sent and summed in bfloat16 or wider, within the bound.
No kernel may reach another device: no remote copies, remote signals or barrier semaphores. Data moves between devices by JAX's collectives and lax.ppermute only.
A program may use at most 64 MiB of HBM per device.

```python
import jax
import jax.numpy as jnp
from jax import lax

D = 2048
CONV_CH = 1024
KERNEL = 31
LAYERS = 3
TOKENS = 24576
N_TP = 4


def draw_conv_taps(key, part):
    first_key, second_key, third_key = jax.random.split(key, 3)
    groups = (CONV_CH + 127) // 128
    group_scale = jnp.exp(jax.random.uniform(second_key, (LAYERS, 1, groups), jnp.float32, -1.0, 1.0))
    group_scale = jnp.repeat(group_scale, 128, axis=2)[:, :, :CONV_CH]
    channel_scale = jnp.exp(jax.random.uniform(third_key, (LAYERS, 1, CONV_CH), jnp.float32, -0.2, 0.2))
    raw_taps = jnp.clip(jax.random.normal(first_key, (LAYERS, KERNEL, CONV_CH), jnp.float32), -4.0, 4.0)
    return (raw_taps * group_scale * channel_scale / jnp.sqrt(float(KERNEL))).astype(jnp.float32)


def steps_of(rng, extent, cuts, smallest, top_value):
    gain = 1.0
    for position, parts in cuts:
        heights = jax.random.uniform(jax.random.fold_in(jax.random.fold_in(rng, 6), position), (parts,), jnp.float32, smallest / len(cuts), top_value / len(cuts))
        gain = gain * jnp.repeat(jnp.exp(heights), extent[position] // parts).reshape((-1,) + (1,) * (len(extent) - 1 - position))
    return gain


def scatter_about(rng, shape, scale, most, shards=(), dtype=jnp.bfloat16):
    level = steps_of(rng, shape, shards, -0.22, 0.18) if shards else 1.0
    result = jax.random.normal(rng, shape, jnp.float32) * scale * level
    return jnp.minimum(jnp.maximum(result, -most), most).astype(dtype)


def setup_inputs(seed: int = 0) -> dict:
    key_list = jax.random.split(jax.random.key(seed), 10)
    return {
        "tokens": scatter_about(key_list[0], (TOKENS, D), 1.0, 6.0, ((0, 64), (1, 4))),
        "norm_gain": jnp.clip(1.0 + 0.18 * jax.random.normal(key_list[1], (LAYERS, D), jnp.float32), 0.1, 1.9),
        "w_value": scatter_about(key_list[2], (LAYERS, D, CONV_CH), D ** -0.5, 0.125, ((1, 64), (2, 4))),
        "w_gate": scatter_about(key_list[3], (LAYERS, D, CONV_CH), D ** -0.5, 0.125, ((1, 64), (2, 4))),
        "conv_taps": draw_conv_taps(jax.random.fold_in(key_list[9], 71), 0),
        "conv_bias": scatter_about(key_list[5], (LAYERS, CONV_CH), 0.5, 3.0, ((1, 4),), jnp.float32),
        "ln_gain": jnp.clip(1.0 + 0.18 * jax.random.normal(key_list[6], (LAYERS, CONV_CH), jnp.float32), 0.1, 1.9),
        "ln_shift": scatter_about(key_list[7], (LAYERS, CONV_CH), 0.5, 3.0, ((1, 4),), jnp.float32),
        "w_out": scatter_about(key_list[8], (LAYERS, CONV_CH, D), CONV_CH ** -0.5, 0.1875, ((1, 4), (2, 64))),
    }


norm_floor = 0.01

def reference(tokens, norm_gain, w_value, w_gate, conv_taps, conv_bias, ln_gain, ln_shift, w_out):
    stream = tokens
    reach = KERNEL // 2
    block_width = CONV_CH // N_TP
    for layer_index in range(LAYERS):
        stream_f32 = stream.astype(jnp.float32)
        scale_rows = lax.rsqrt(lax.optimization_barrier(jnp.mean(stream_f32 * stream_f32, axis=-1, keepdims=True)) + norm_floor)
        normed = (stream_f32 * scale_rows * norm_gain[layer_index]).astype(jnp.bfloat16)
        value_rows = jnp.dot(normed, w_value[layer_index], preferred_element_type=jnp.float32)
        gate_rows = jnp.dot(normed, w_gate[layer_index], preferred_element_type=jnp.float32)
        gated_input = (value_rows * jax.nn.sigmoid(gate_rows)).astype(jnp.bfloat16)
        padded = jnp.pad(gated_input, ((reach, reach), (0, 0))).astype(jnp.float32)
        convolved = jnp.zeros((TOKENS, CONV_CH), jnp.float32) + conv_bias[layer_index]
        for offset in range(KERNEL):
            convolved = convolved + conv_taps[layer_index, offset] * padded[offset:offset + TOKENS]
        average = lax.optimization_barrier(jnp.mean(convolved, axis=-1, keepdims=True))
        spread = lax.optimization_barrier(jnp.mean(convolved * convolved, axis=-1, keepdims=True)) - average * average
        activated = jax.nn.silu((convolved - average) * lax.rsqrt(spread + norm_floor) * ln_gain[layer_index] + ln_shift[layer_index]).astype(jnp.bfloat16)
        summed = jnp.zeros((TOKENS, D), jnp.float32)
        for block_index in range(N_TP):
            first = block_index * block_width
            partial_block = jnp.dot(activated[:, first:first + block_width], w_out[layer_index, first:first + block_width], preferred_element_type=jnp.float32).astype(jnp.bfloat16)
            partial_block = lax.optimization_barrier(partial_block)
            summed = summed + partial_block.astype(jnp.float32)
        stream = (stream_f32 + summed).astype(jnp.bfloat16)
    return stream
```

```python
import functools

import jax
import jax.numpy as jnp
from jax import lax
from jax.experimental import pallas as pl
from jax.experimental.pallas import tpu as pltpu
from jax.sharding import Mesh
from jax.sharding import PartitionSpec as P

SP = ("z", "y", "c")
EDGE = 16
LANES = 128
norm_floor = 0.01
bf16, f32 = jnp.bfloat16, jnp.float32


def to_all(array, axis):
    copies = jnp.broadcast_to(array, (lax.axis_size(axis), *array.shape))
    return lax.all_to_all(copies, axis, split_axis=0, concat_axis=0, tiled=True)


def core_swap(array):
    return lax.ppermute(array, "c", [(0, 1), (1, 0)])


def after(array, *others):
    return lax.optimization_barrier((array, *others))[0]


def place_rows(core, pieces, store):
    n_y, n_z, n_i, _ = pieces[0].shape

    def step(z, carry):
        for y in range(n_y):
            for piece, c in zip(pieces, (core, 1 - core)):
                row = pl.multiple_of(((z * n_y + y) * 2 + c) * n_i, n_i)
                store(pl.ds(row, n_i), piece[y, z])
        return carry

    lax.fori_loop(0, n_z, step, 0)


def up_kernel(layer, total, info, stream, gain, own, other, out, weights, normed):
    n_x, rows, width = stream.shape
    ch = out.shape[-1]

    def store(where, value):
        weights[where, :] = value

    place_rows(info[0], (own, other), store)
    squares = jnp.zeros((rows, 1), f32)
    for b in range(n_x):
        block = stream[b].astype(f32)
        squares += jnp.sum(block * block, axis=-1, keepdims=True)
    scale = lax.rsqrt(squares * (1.0 / (n_x * width)) + norm_floor)
    for b in range(n_x):
        lanes = slice(b * width, (b + 1) * width)
        block = stream[b].astype(f32)
        normed[:, lanes] = (block * scale * gain[layer : layer + 1, lanes]).astype(bf16)
    both = jnp.dot(normed[...], weights[...], preferred_element_type=f32)
    gated = both[:, :ch] * jax.nn.sigmoid(both[:, ch:])
    t = info[2 + layer] + lax.broadcasted_iota(jnp.int32, (rows, 1), 0)
    gated = jnp.where((t >= 0) & (t < total), gated, 0.0).astype(bf16)
    for b in range(out.shape[0]):
        out[b] = gated


def down_kernel(layer, last, info, gated, par, own, other, stream, out, weights, act, conv):
    n_x, rows, ch = gated.shape
    keep = rows - 2 * EDGE
    taps = par.shape[2] - 3
    shift = EDGE - taps // 2
    step_rows = 64 if keep % 64 == 0 else 32
    window = step_rows + 2 * EDGE
    strips = [(x, s) for x in range(n_x) for s in range(0, ch, LANES)]
    inverse = 1.0 / (n_x * ch)

    for x in range(n_x):

        def store(where, value, x=x):
            weights[where, x * ch : (x + 1) * ch] = value

        place_rows(info[0], (own.at[x], other.at[x]), store)

    def chunk(i, carry):
        first = pl.multiple_of(i * step_rows, step_rows)
        total = jnp.zeros((step_rows, LANES), f32)
        squares = jnp.zeros((step_rows, LANES), f32)
        for x, s in strips:
            lanes = slice(s, s + LANES)
            win = gated[x, pl.ds(first, window), lanes].astype(f32)
            acc = jnp.zeros((step_rows, LANES), f32) + par[x, layer, taps : taps + 1, lanes]
            for r in range(8):
                turned = pltpu.roll(win, window - r, 0) if r else win
                for q in range(window // 8):
                    k = 8 * q + r - shift
                    if 0 <= k < taps:
                        tap = par[x, layer, k : k + 1, lanes]
                        acc = acc + tap * turned[8 * q : 8 * q + step_rows]
            conv[:, x * ch + s : x * ch + s + LANES] = acc
            total = total + acc
            squares = squares + acc * acc
        average = jnp.sum(total, axis=-1, keepdims=True) * inverse
        spread = jnp.sum(squares, axis=-1, keepdims=True) * inverse - average * average
        scale = lax.rsqrt(spread + norm_floor)
        for x, s in strips:
            lanes = slice(s, s + LANES)
            wide = slice(x * ch + s, x * ch + s + LANES)
            value = (conv[:, wide] - average) * scale
            value = value * par[x, layer, taps + 1 : taps + 2, lanes] + par[x, layer, taps + 2 : taps + 3, lanes]
            act[pl.ds(first, step_rows), wide] = (value * jax.nn.sigmoid(value)).astype(bf16)
        return carry

    lax.fori_loop(0, keep // step_rows, chunk, 0)
    width = stream.shape[2]
    dims = (((1,), (1,)), ((), ()))
    if last:
        added = lax.dot_general(act[...], weights[...], dims, preferred_element_type=f32)
        base = stream[info[1], EDGE : EDGE + keep].astype(f32)
        out[...] = (base + added).astype(bf16)
    else:
        for b in range(n_x):
            part = weights[b * width : (b + 1) * width]
            added = lax.dot_general(act[...], part, dims, preferred_element_type=f32)
            out[b] = (stream[b, EDGE : EDGE + keep].astype(f32) + added).astype(bf16)


def in_vmem(count):
    return [pl.BlockSpec(memory_space=pltpu.SMEM)] + [pl.BlockSpec(memory_space=pltpu.VMEM)] * count


def up(layer, total, info, stream, gain, own, other):
    n_x, rows, width = stream.shape
    pair = own.shape[-1]
    return pl.pallas_call(
        functools.partial(up_kernel, layer, total),
        out_shape=jax.ShapeDtypeStruct((n_x, rows, pair // 2), bf16),
        in_specs=in_vmem(4),
        out_specs=pl.BlockSpec(memory_space=pltpu.VMEM),
        scratch_shapes=[
            pltpu.VMEM((n_x * width, pair), bf16),
            pltpu.VMEM((rows, n_x * width), bf16),
        ],
        name=f"up_{layer}",
    )(info, stream, gain, own, other)


def down(layer, last, info, gated, par, own, other, stream):
    n_x, rows, ch = gated.shape
    keep = rows - 2 * EDGE
    width = stream.shape[2]
    features = width if last else n_x * width
    step_rows = 64 if keep % 64 == 0 else 32
    shape = (keep, width) if last else (n_x, keep, width)
    return pl.pallas_call(
        functools.partial(down_kernel, layer, last),
        out_shape=jax.ShapeDtypeStruct(shape, bf16),
        in_specs=in_vmem(5),
        out_specs=pl.BlockSpec(memory_space=pltpu.VMEM),
        scratch_shapes=[
            pltpu.VMEM((features, n_x * ch), bf16),
            pltpu.VMEM((keep, n_x * ch), bf16),
            pltpu.VMEM((step_rows, n_x * ch), f32),
        ],
        name=f"down_{layer}",
    )(info, gated, par, own, other, stream)


def body(tokens, norm_gain, w_value, w_gate, conv_taps, conv_bias, ln_gain, ln_shift, w_out):
    layers, n_i, ch = w_value.shape
    n_x = lax.axis_size("x")
    n_tok, f_loc = tokens.shape
    halo = EDGE * layers
    size = lax.axis_size(SP)
    total = size * n_tok
    place = lax.axis_index(SP) * n_tok
    info = jnp.stack(
        [lax.axis_index("c"), lax.axis_index("x")] + [place - EDGE * (layers - l) for l in range(layers)]
    ).astype(jnp.int32)

    before = lax.ppermute(tokens[n_tok - halo :], SP, [(i, i + 1) for i in range(size - 1)])
    behind = lax.ppermute(tokens[:halo], SP, [(i + 1, i) for i in range(size - 1)])
    stream = to_all(jnp.concatenate([before, tokens, behind], axis=0), "x")

    par = jnp.concatenate([conv_taps, conv_bias[:, None], ln_gain[:, None], ln_shift[:, None]], axis=1)
    par = to_all(par, "x")

    out_t = jnp.swapaxes(w_out, 1, 2)
    ups, outs = [], []
    for l in range(layers):
        outward = to_all(to_all(out_t[l], "z"), "y")
        inward = to_all(to_all(jnp.concatenate([w_value[l], w_gate[l]], axis=1), "z"), "y")
        if l < layers - 1:
            outward = to_all(outward, "x")
        else:
            n_y, n_z = outward.shape[:2]
            by_x = jnp.moveaxis(outward.reshape(n_y, n_x, n_z // n_x, n_i, ch), 1, 0)
            outward = lax.all_to_all(by_x, "x", split_axis=0, concat_axis=0, tiled=True)
        ups.append((inward, core_swap(inward)))
        outs.append((outward, core_swap(outward)))

    for l in range(layers):
        gated = up(l, total, info, stream, norm_gain, *ups[l])
        gated = lax.all_to_all(gated, "x", split_axis=0, concat_axis=0, tiled=True)
        stream = down(l, l == layers - 1, info, gated, par, *outs[l], stream)
    return stream


def solution(mesh):
    torus = Mesh(mesh.devices.reshape(8, 4, 2, mesh.shape["tp"]), ("z", "y", "c", "x"))
    return jax.shard_map(
        body,
        mesh=torus,
        in_specs=(
            P(SP, "x"),
            P(),
            P(None, SP, "x"),
            P(None, SP, "x"),
            P(None, None, "x"),
            P(None, "x"),
            P(None, "x"),
            P(None, "x"),
            P(None, "x", SP),
        ),
        out_specs=P(SP, "x"),
        check_vma=False,
    )
```

```python
import functools

import jax
import jax.numpy as jnp
from jax import lax
from jax.experimental import pallas as pl
from jax.experimental.pallas import tpu as pltpu
from jax.sharding import Mesh
from jax.sharding import PartitionSpec as P

SP = ("z", "y", "c")
EDGE = 16
LANES = 128
norm_floor = 0.01
bf16, f32 = jnp.bfloat16, jnp.float32


def to_all(array, axis):
    copies = jnp.broadcast_to(array, (lax.axis_size(axis), *array.shape))
    return lax.all_to_all(copies, axis, split_axis=0, concat_axis=0, tiled=True)


def shifted(array, axis, s):
    n = lax.axis_size(axis)
    return lax.ppermute(array, axis, [(i, (i + s) % n) for i in range(n)])


def spread(array, axis):
    n = lax.axis_size(axis)
    pieces = {s: shifted(array, axis, s) for s in (1, n - 1, *range(2, n - 1))}
    return [array] + [pieces[s] for s in range(1, n)]


def swap(array):
    return shifted(array, "c", 1)


def behind(position, s, n):
    return lax.rem(position + (n - s), n)


def place_rows(info, n_y, sources, weights, columns):
    core, _, my_y = info[0], info[1], info[2]
    n_z, n_i = sources[0][2], sources[0][3]

    def step(z, carry):
        for s, (own, other, _, _) in enumerate(sources):
            y = behind(my_y, s, n_y)
            for piece, c in ((own, core), (other, 1 - core)):
                row = pl.multiple_of(((z * n_y + y) * 2 + c) * n_i, n_i)
                weights[pl.ds(row, n_i), columns] = piece(z)
        return carry

    lax.fori_loop(0, n_z, step, 0)


def up_kernel(layer, total, n_s, n_y, info, *refs):
    streams, refs = refs[:n_s], refs[n_s:]
    gain, par, refs = refs[0], refs[1], refs[2:]
    owns, others, refs = refs[:n_y], refs[n_y : 2 * n_y], refs[2 * n_y :]
    out, weights, normed, padded, conv = refs
    n_x, rows, width = normed.shape
    keep = rows - 2 * EDGE
    ch = out.shape[-1]
    taps = par.shape[1] - 3
    shift = EDGE - taps // 2
    n_z, n_i = owns[0].shape[:2]
    my_x = info[1]

    def wide(ref):
        return lambda z: ref[z, :, : 2 * ch]

    place_rows(info, n_y, [(wide(a), wide(b), n_z, n_i) for a, b in zip(owns, others)], weights, slice(0, 2 * ch))

    def block(s):
        b = behind(my_x, s, n_x)
        return b, (streams[s][...] if n_s > 1 else streams[0][b]).astype(f32)

    squares = jnp.zeros((rows, 1), f32)
    for s in range(n_x):
        _, value = block(s)
        squares += jnp.sum(value * value, axis=-1, keepdims=True)
    scale = lax.rsqrt(squares * (1.0 / (n_x * width)) + norm_floor)
    for s in range(n_x):
        b, value = block(s)
        normed[b] = (value * scale * gain[layer, pl.ds(b, 1), :]).astype(bf16)
    both = jnp.zeros((rows, 2 * ch), f32)
    for b in range(n_x):
        both += jnp.dot(normed[b], weights[b * width : (b + 1) * width], preferred_element_type=f32)
    gated = both[:, :ch] * jax.nn.sigmoid(both[:, ch:])
    t = info[3 + layer] + lax.broadcasted_iota(jnp.int32, (rows, 1), 0)
    padded[...] = jnp.where((t >= 0) & (t < total), gated, 0.0).astype(bf16).astype(f32)

    step_rows = 64 if keep % 64 == 0 else 32
    window = step_rows + 2 * EDGE

    def chunk(i, carry):
        first = pl.multiple_of(i * step_rows, step_rows)
        for lane in range(0, ch, LANES):
            lanes = slice(lane, lane + LANES)
            win = padded[pl.ds(first, window), lanes]
            acc = jnp.zeros((step_rows, LANES), f32) + par[layer, taps : taps + 1, lanes]
            for r in range(8):
                turned = pltpu.roll(win, window - r, 0) if r else win
                for q in range(window // 8):
                    k = 8 * q + r - shift
                    if 0 <= k < taps:
                        acc = acc + par[layer, k : k + 1, lanes] * turned[8 * q : 8 * q + step_rows]
            conv[pl.ds(first, step_rows), lanes] = acc
        return carry

    lax.fori_loop(0, keep // step_rows, chunk, 0)
    values = conv[...]
    mean = jnp.sum(values, axis=-1, keepdims=True) * (1.0 / ch)
    centred = (values - mean).astype(bf16)
    high = mean.astype(bf16).astype(f32)
    low = mean - high
    lane = lax.broadcasted_iota(jnp.int32, (keep, LANES), 1)
    columns = jnp.where(lane == 0, high, jnp.where(lane == 1, low, 0.0))
    columns = jnp.concatenate([columns, jnp.zeros((2 * ch - keep, LANES), f32)], axis=0)
    across = columns.T[:8]
    tail = jnp.concatenate([across[:, :ch], across[:, ch:]], axis=0).astype(bf16)
    for b in range(out.shape[0]):
        out[b, :keep] = centred
        out[b, keep:] = tail


def down_kernel(layer, last, n_s, n_y, n_x, info, *refs):
    gated, par, refs = refs[0], refs[1], refs[2:]
    streams, refs = refs[:n_s], refs[n_s:]
    owns, others, refs = refs[:n_y], refs[n_y : 2 * n_y], refs[2 * n_y :]
    far, far_other, refs = refs[: n_x - 1], refs[n_x - 1 : 2 * n_x - 2], refs[2 * n_x - 2 :]
    out, weights, act = refs
    _, rows, ch = gated.shape
    keep = rows - EDGE
    my_x = info[1]
    n_i = owns[0].shape[1]
    n_z = far[0].shape[1]
    width = out.shape[-1]

    def near(ref):
        return lambda z: ref[z + (my_x * n_z if last else 0), :, 2 * ch :]

    def away(ref, s):
        return lambda z: ref[s, z]

    place_rows(info, n_y, [(near(a), near(b), n_z, n_i) for a, b in zip(owns, others)], weights, slice(0, ch))
    for s in range(1, n_x):
        sources = [(away(far[s - 1], q), away(far_other[s - 1], q), n_z, n_i) for q in range(n_y)]
        place_rows(info, n_y, sources, weights, slice(s * ch, (s + 1) * ch))

    order = [behind(my_x, s, n_x) for s in range(n_x)]
    tails = [gated[b, keep:].astype(f32) for b in order]
    spans = [jnp.concatenate([v[:8], v[8:]], axis=1) for v in tails]
    across = jnp.concatenate(spans + [jnp.zeros((LANES - 8 * n_x, 2 * ch), f32)], axis=0)
    columns = across.T[:keep]
    means = [columns[:, 8 * s : 8 * s + 1] + columns[:, 8 * s + 1 : 8 * s + 2] for s in range(n_x)]
    average = sum(means) * (1.0 / n_x)
    offsets = [m - average for m in means]
    squares = jnp.zeros((keep, ch), f32)
    for s, b in enumerate(order):
        value = gated[b, :keep].astype(f32) + offsets[s]
        squares += value * value
    spread_rows = jnp.sum(squares, axis=-1, keepdims=True) * (1.0 / (n_x * ch))
    scale = lax.rsqrt(spread_rows + norm_floor)
    taps = par.shape[2] - 3
    for s, b in enumerate(order):
        value = (gated[b, :keep].astype(f32) + offsets[s]) * scale
        value = value * par[b, layer, taps + 1 : taps + 2, :] + par[b, layer, taps + 2 : taps + 3, :]
        act[:, s * ch : (s + 1) * ch] = (value * jax.nn.sigmoid(value)).astype(bf16)

    dims = (((1,), (1,)), ((), ()))
    inner = slice(EDGE, EDGE + keep)
    if last:
        added = lax.dot_general(act[...], weights[...], dims, preferred_element_type=f32)
        out[...] = (streams[0][my_x, inner].astype(f32) + added).astype(bf16)
    else:
        for s, b in enumerate(order):
            part = weights[pl.ds(pl.multiple_of(b * width, width), width), :]
            added = lax.dot_general(act[...], part, dims, preferred_element_type=f32)
            base = streams[s][inner] if n_s > 1 else streams[0][b, inner]
            out[b] = (base.astype(f32) + added).astype(bf16)


def vmem():
    return pl.BlockSpec(memory_space=pltpu.VMEM)


def smem():
    return pl.BlockSpec(memory_space=pltpu.SMEM)


def up(layer, total, info, streams, gain, par, owns, others, ch):
    n_x = lax.axis_size("x")
    rows, width = streams[0].shape[-2:]
    keep = rows - 2 * EDGE
    return pl.pallas_call(
        functools.partial(up_kernel, layer, total, len(streams), len(owns)),
        out_shape=jax.ShapeDtypeStruct((n_x, keep + EDGE, ch), bf16),
        in_specs=[smem()]
        + [vmem()] * (len(streams) + 2)
        + [vmem()] * (len(owns) + len(others)),
        out_specs=vmem(),
        scratch_shapes=[
            pltpu.VMEM((n_x * width, 2 * ch), bf16),
            pltpu.VMEM((n_x, rows, width), bf16),
            pltpu.VMEM((rows, ch), f32),
            pltpu.VMEM((keep, ch), f32),
        ],
        name=f"up_{layer}",
    )(info, *streams, gain, par, *owns, *others)


def down(layer, last, info, gated, par, streams, owns, others, far, far_other):
    n_x, rows, ch = gated.shape
    keep = rows - EDGE
    width = streams[0].shape[-1]
    features = width if last else n_x * width
    shape = (keep, width) if last else (n_x, keep, width)
    return pl.pallas_call(
        functools.partial(down_kernel, layer, last, len(streams), len(owns), n_x),
        out_shape=jax.ShapeDtypeStruct(shape, bf16),
        in_specs=[smem()]
        + [vmem()] * (len(streams) + 2)
        + [vmem()] * (len(owns) + len(others) + len(far) + len(far_other)),
        out_specs=vmem(),
        scratch_shapes=[pltpu.VMEM((features, n_x * ch), bf16), pltpu.VMEM((keep, n_x * ch), bf16)],
        name=f"down_{layer}",
    )(info, gated, par, *streams, *owns, *others, *far, *far_other)


def body(tokens, norm_gain, w_value, w_gate, conv_taps, conv_bias, ln_gain, ln_shift, w_out):
    layers, n_i, ch = w_value.shape
    n_x = lax.axis_size("x")
    my_x = lax.axis_index("x")
    n_tok, f_loc = tokens.shape
    halo = EDGE * layers
    size = lax.axis_size(SP)
    total = size * n_tok
    place = lax.axis_index(SP) * n_tok
    info = jnp.stack(
        [lax.axis_index("c"), my_x, lax.axis_index("y")]
        + [place - EDGE * (layers - l) for l in range(layers)]
    ).astype(jnp.int32)
    gain = norm_gain.reshape(layers, n_x, f_loc)

    before = lax.ppermute(tokens[n_tok - halo :], SP, [(i, i + 1) for i in range(size - 1)])
    following = lax.ppermute(tokens[:halo], SP, [(i + 1, i) for i in range(size - 1)])
    streams = spread(jnp.concatenate([before, tokens, following], axis=0), "x")

    par = jnp.concatenate([conv_taps, conv_bias[:, None], ln_gain[:, None], ln_shift[:, None]], axis=1)
    pars = to_all(par, "x")

    out_t = jnp.swapaxes(w_out, 1, 2)
    weights = []
    for l in range(layers):
        pack = jnp.concatenate([w_value[l], w_gate[l], out_t[l]], axis=1)
        owns = spread(to_all(pack, "z"), "y")
        others = [swap(a) for a in owns]
        outward = jnp.stack([a[..., 2 * ch :] for a in owns])
        if l < layers - 1:
            far = spread(outward, "x")[1:]
        else:
            part = outward.shape[1] // n_x
            far = [
                shifted(lax.dynamic_slice_in_dim(outward, lax.rem(my_x + s, n_x) * part, part, axis=1), "x", s)
                for s in range(1, n_x)
            ]
        far_other = [swap(a) for a in far]
        weights.append((owns, others, far, far_other))

    for l in range(layers):
        owns, others, far, far_other = weights[l]
        gated = up(l, total, info, streams, gain, par, owns, others, ch)
        gated = lax.all_to_all(gated, "x", split_axis=0, concat_axis=0, tiled=True)
        stream = down(l, l == layers - 1, info, gated, pars, streams, owns, others, far, far_other)
        streams = [stream]
    return stream


def solution(mesh):
    torus = Mesh(mesh.devices.reshape(8, 4, 2, mesh.shape["tp"]), ("z", "y", "c", "x"))
    return jax.shard_map(
        body,
        mesh=torus,
        in_specs=(
            P(SP, "x"),
            P(),
            P(None, SP, "x"),
            P(None, SP, "x"),
            P(None, None, "x"),
            P(None, "x"),
            P(None, "x"),
            P(None, "x"),
            P(None, "x", SP),
        ),
        out_specs=P(SP, "x"),
        check_vma=False,
    )
```

```python
import functools

import jax
import jax.numpy as jnp
from jax import lax
from jax.experimental import pallas as pl
from jax.experimental.pallas import tpu as pltpu
from jax.sharding import Mesh
from jax.sharding import PartitionSpec as P


SP = ("z", "y", "c")
EDGE = 16
LANES = 128
norm_floor = 0.01
bf16, f32 = jnp.bfloat16, jnp.float32


def to_all(array, axis):
    copies = jnp.broadcast_to(array, (lax.axis_size(axis), *array.shape))
    return lax.all_to_all(copies, axis, split_axis=0, concat_axis=0, tiled=True)


def shifted(array, axis, s):
    n = lax.axis_size(axis)
    return lax.ppermute(array, axis, [(i, (i + s) % n) for i in range(n)])


def spread(array, axis):
    n = lax.axis_size(axis)
    pieces = {s: shifted(array, axis, s) for s in (n // 2, 1, n - 1)}
    return [array] + [pieces[s] for s in range(1, n)]


def swap(arrays):
    return [shifted(a, "c", 1) for a in arrays]


def after(arrays, *others):
    return lax.optimization_barrier((tuple(arrays), *others))[0]


def behind(position, s, n):
    return lax.rem(position + (n - s), n)


def row_step(rows):
    return 64 if rows % 64 == 0 else 32


def up_kernel(layer, total, n_s, n_y, first_lane, info, *refs):
    streams, refs = refs[:n_s], refs[n_s:]
    gain, par, refs = refs[0], refs[1], refs[2:]
    pieces, refs = refs[:-7], refs[-7:]
    out, weights, normed, both, padded, columns, sems = refs
    rows, features = normed.shape
    n_x, width = gain.shape[1:]
    keep = rows - 2 * EDGE
    ch = out.shape[-1]
    taps = par.shape[1] - 3
    shift = EDGE - taps // 2
    core, my_x, my_y = info[0], info[1], info[2]

    if n_y:
        copies = []
        for i, piece in enumerate(pieces):
            c = core if i < n_y else 1 - core
            rows_of = weights.at[:, behind(my_y, i % n_y, n_y), c]
            copies.append(pltpu.make_async_copy(piece, rows_of, sems.at[i]))
    else:
        copies = [pltpu.make_async_copy(pieces[0].at[:, pl.ds(first_lane, 2 * ch)], weights, sems.at[0])]
    for copy in copies:
        copy.start()

    step = 32

    def norm(i, carry):
        here = pl.ds(pl.multiple_of(i * step, step), step)
        squares = jnp.zeros((step, width), f32)
        for s in range(n_x):
            value = (streams[s][here] if n_s > 1 else streams[0][s, here]).astype(f32)
            squares += value * value
        mean = jnp.sum(squares, axis=-1, keepdims=True) * (1.0 / features)
        scale = lax.rsqrt(mean + norm_floor)
        for s in range(n_x):
            b = behind(my_x, s, n_x) if n_s > 1 else s
            value = (streams[s][here] if n_s > 1 else streams[0][s, here]).astype(f32)
            value = (value * scale * gain[layer, pl.ds(b, 1), :]).astype(bf16)
            normed[here, pl.ds(pl.multiple_of(b * width, width), width)] = value
        return carry

    lax.fori_loop(0, rows // step, norm, 0)
    for copy in copies:
        copy.wait()
    for half in range(2):
        part = weights[..., half * ch : (half + 1) * ch].reshape(features, ch)
        both[half] = jnp.dot(normed[...], part, preferred_element_type=f32)

    def gate(i, carry):
        first = pl.multiple_of(i * step, step)
        here = pl.ds(first, step)
        gated = both[0, here] * jax.nn.sigmoid(both[1, here])
        t = info[3 + layer] + first + lax.broadcasted_iota(jnp.int32, (step, 1), 0)
        gated = jnp.where((t >= 0) & (t < total), gated, 0.0).astype(bf16)
        padded[here] = gated.astype(f32)
        return carry

    lax.fori_loop(0, rows // step, gate, 0)

    size = row_step(keep)
    window = size + 2 * EDGE
    lane = lax.broadcasted_iota(jnp.int32, (size, LANES), 1)
    columns[pl.ds(keep, 2 * ch - keep)] = jnp.zeros((2 * ch - keep, LANES), f32)

    def chunk(i, carry):
        first = pl.multiple_of(i * size, size)
        accs = []
        for start in range(0, ch, LANES):
            lanes = slice(start, start + LANES)
            win = padded[pl.ds(first, window), lanes]
            acc = jnp.zeros((size, LANES), f32) + par[layer, taps : taps + 1, lanes]
            for r in range(8):
                turned = pltpu.roll(win, window - r, 0) if r else win
                for q in range(window // 8):
                    k = 8 * q + r - shift
                    if 0 <= k < taps:
                        acc = acc + par[layer, k : k + 1, lanes] * turned[8 * q : 8 * q + size]
            accs.append(acc)
        mean = jnp.sum(sum(accs), axis=-1, keepdims=True) * (1.0 / ch)
        for start, acc in zip(range(0, ch, LANES), accs):
            out[pl.ds(first, size), start : start + LANES] = (acc - mean).astype(bf16)
        high = mean.astype(bf16).astype(f32)
        columns[pl.ds(first, size)] = jnp.where(lane == 0, high, jnp.where(lane == 1, mean - high, 0.0))
        return carry

    lax.fori_loop(0, keep // size, chunk, 0)
    across = columns[...].T[:8]
    tail = jnp.concatenate([across[:, :ch], across[:, ch:]], axis=0).astype(bf16)
    out[keep:] = tail


def down_kernel(layer, last, n_s, n_y, n_x, first_lane, info, *refs):
    gated, refs = refs[:n_x], refs[n_x:]
    pars, refs = refs[:n_x], refs[n_x:]
    streams, refs = refs[:n_s], refs[n_s:]
    pieces, refs = refs[:-5], refs[-5:]
    out, weights, act, columns, sems = refs
    rows, ch = gated[0].shape
    keep = rows - EDGE
    core, my_x, my_y = info[0], info[1], info[2]
    width = out.shape[-1]

    copies = []

    def fetch(source, to):
        copies.append(pltpu.make_async_copy(source, to, sems.at[len(copies)]))

    if n_y:
        for i, piece in enumerate(pieces):
            c = core if i < n_y else 1 - core
            fetch(piece, weights.at[:, behind(my_y, i % n_y, n_y), c])
    elif last:
        mine = pl.ds(pl.multiple_of(my_x * width, width), width)
        fetch(pieces[0].at[mine, pl.ds(first_lane, ch)], weights.at[:, pl.ds(0, ch)])
        for s in range(1, n_x):
            fetch(pieces[s], weights.at[:, pl.ds(s * ch, ch)])
    else:
        fetch(pieces[0].at[:, pl.ds(first_lane, n_x * ch)], weights)
    for copy in copies:
        copy.start()

    spans = []
    for s in range(n_x):
        tail = gated[s][keep:].astype(f32)
        spans.append(jnp.concatenate([tail[:8], tail[8:]], axis=1))
    spans.append(jnp.zeros((LANES - 8 * n_x, 2 * ch), f32))
    columns[...] = jnp.concatenate(spans, axis=0).T

    size = row_step(keep)

    def chunk(i, carry):
        here = pl.ds(pl.multiple_of(i * size, size), size)
        cols = columns[here]
        means = [cols[:, 8 * s : 8 * s + 1] + cols[:, 8 * s + 1 : 8 * s + 2] for s in range(n_x)]
        average = sum(means) * (1.0 / n_x)
        squares = jnp.zeros((size, ch), f32)
        for s in range(n_x):
            value = gated[s][here].astype(f32) + (means[s] - average)
            squares += value * value
        mean = jnp.sum(squares, axis=-1, keepdims=True) * (1.0 / (n_x * ch))
        scale = lax.rsqrt(mean + norm_floor)
        for s in range(n_x):
            value = (gated[s][here].astype(f32) + (means[s] - average)) * scale
            value = value * pars[s][layer, 0:1, :] + pars[s][layer, 1:2, :]
            act[here, s * ch : (s + 1) * ch] = (value * jax.nn.sigmoid(value)).astype(bf16)
        return carry

    lax.fori_loop(0, keep // size, chunk, 0)
    for copy in copies:
        copy.wait()
    dims = (((1,), (1,)), ((), ()))
    inner = slice(EDGE, EDGE + keep)
    if last:
        added = lax.dot_general(act[...], weights[...], dims, preferred_element_type=f32)
        out[...] = (streams[0][my_x, inner].astype(f32) + added).astype(bf16)
    else:
        part_rows = weights.shape[0] // n_x

        def block(b, base):
            part = weights[pl.ds(b * part_rows, part_rows)].reshape(width, n_x * ch)
            added = lax.dot_general(act[...], part, dims, preferred_element_type=f32)
            out[b] = (base.astype(f32) + added).astype(bf16)

        if n_s > 1:
            for s in range(n_x):
                block(behind(my_x, s, n_x), streams[s][inner])
        else:
            lax.fori_loop(0, n_x, lambda b, carry: (block(b, streams[0][b, inner]), carry)[1], 0)


def vmem():
    return pl.BlockSpec(memory_space=pltpu.VMEM)


def hbm():
    return pl.BlockSpec(memory_space=pltpu.HBM)


def smem():
    return pl.BlockSpec(memory_space=pltpu.SMEM)


def up(layer, total, info, streams, gain, par, pieces, ch, first_lane=0):
    n_x, width = gain.shape[1:]
    rows = streams[0].shape[-2]
    keep = rows - 2 * EDGE
    n_y = len(pieces) // 2
    shape = (n_x * width,)
    if n_y:
        n_z, n_i, _ = pieces[0].shape
        shape = (n_z, n_y, 2, n_i)
    return pl.pallas_call(
        functools.partial(up_kernel, layer, total, len(streams), n_y, first_lane),
        out_shape=jax.ShapeDtypeStruct((keep + EDGE, ch), bf16),
        in_specs=[smem()] + [vmem()] * (len(streams) + 2) + [hbm()] * len(pieces),
        out_specs=vmem(),
        scratch_shapes=[
            pltpu.VMEM((*shape, 2 * ch), bf16),
            pltpu.VMEM((rows, n_x * width), bf16),
            pltpu.VMEM((2, rows, ch), f32),
            pltpu.VMEM((rows, ch), f32),
            pltpu.VMEM((2 * ch, LANES), f32),
            pltpu.SemaphoreType.DMA((len(pieces),)),
        ],
    )(info, *streams, gain, par, *pieces)


def down(layer, last, info, gated, pars, streams, pieces, paired, first_lane=0):
    rows, ch = gated[0].shape
    n_x = len(gated)
    keep = rows - EDGE
    width = streams[0].shape[-1]
    n_y = len(pieces) // 2 if paired else 0
    shape = (width if last else n_x * width,)
    if paired:
        n_z, n_i, _ = pieces[0].shape
        shape = (n_z, n_y, 2, n_i)
    out_shape = (keep, width) if last else (n_x, keep, width)
    return pl.pallas_call(
        functools.partial(down_kernel, layer, last, len(streams), n_y, n_x, first_lane),
        out_shape=jax.ShapeDtypeStruct(out_shape, bf16),
        in_specs=[smem()] + [vmem()] * (2 * n_x + len(streams)) + [hbm()] * len(pieces),
        out_specs=vmem(),
        scratch_shapes=[
            pltpu.VMEM((*shape, n_x * ch), bf16),
            pltpu.VMEM((keep, n_x * ch), bf16),
            pltpu.VMEM((2 * ch, LANES), f32),
            pltpu.SemaphoreType.DMA((len(pieces),)),
        ],
    )(info, *gated, *pars, *streams, *pieces)


def program(tokens, norm_gain, w_value, w_gate, conv_taps, conv_bias, ln_gain, ln_shift, w_out):
    layers, _, ch = w_value.shape
    n_x = lax.axis_size("x")
    my_x = lax.axis_index("x")
    n_tok, f_loc = tokens.shape
    halo = EDGE * layers
    size = lax.axis_size(SP)
    total = size * n_tok
    place = lax.axis_index(SP) * n_tok
    info = jnp.stack(
        [lax.axis_index("c"), my_x, lax.axis_index("y")]
        + [place - EDGE * (layers - l) for l in range(layers)]
    ).astype(jnp.int32)
    gain = norm_gain.reshape(layers, n_x, f_loc)

    before = lax.ppermute(tokens[n_tok - halo :], SP, [(i, i + 1) for i in range(size - 1)])
    following = lax.ppermute(tokens[:halo], SP, [(i + 1, i) for i in range(size - 1)])
    streams = spread(jnp.concatenate([before, tokens, following], axis=0), "x")

    par = jnp.concatenate([conv_taps, conv_bias[:, None], ln_gain[:, None], ln_shift[:, None]], axis=1)
    pars = spread(jnp.stack([ln_gain, ln_shift], axis=1), "x")

    info = after([info], *pars[1:])[0]

    out_t = jnp.swapaxes(w_out, 1, 2)
    wide = jnp.concatenate(spread(out_t[: layers - 1], "x"), axis=-1)

    packs, lanes, at = [], [], 0
    for l in range(1, layers):
        packs += [w_value[l], w_gate[l], out_t[l] if l == layers - 1 else wide[l]]
        lanes.append((at, at + 2 * ch))
        at += sum(a.shape[1] for a in packs[-3:])
    rest = lax.all_gather(jnp.concatenate(packs, axis=1), SP, axis=0, tiled=True)

    up_first = to_all(jnp.concatenate([w_value[0], w_gate[0]], axis=1), "z")
    up_first = spread(up_first, "y")
    out_first = to_all(wide[0], "z")
    out_first = spread(out_first, "y")

    for l in range(layers):
        last = l == layers - 1
        if l == 0:
            gated = up(l, total, info, streams, gain, par, [*up_first, *swap(up_first)], ch)
            start = 0
        else:
            first, start = lanes[l - 1]
            gated = up(l, total, info, streams, gain, par, [rest], ch, first)
            pieces = [rest]
        gated = spread(gated, "x")
        if l == 0:
            pieces = after(out_first, *gated[1:])
            pieces = [*pieces, *swap(pieces)]
        if last:
            for s in (1, n_x // 2, n_x - 1):
                row = lax.rem(my_x + s, n_x) * f_loc
                block = lax.dynamic_slice(rest, (row, start), (f_loc, ch))
                pieces.append(shifted(block, "x", s))
        stream = down(l, last, info, gated, pars, streams, pieces, l == 0, start)
        streams = [stream]
    return stream


def solution(mesh):
    torus = Mesh(mesh.devices.reshape(8, 4, 2, mesh.shape["tp"]), ("z", "y", "c", "x"))
    return jax.shard_map(
        program,
        mesh=torus,
        in_specs=(
            P(SP, "x"),
            P(),
            P(None, SP, "x"),
            P(None, SP, "x"),
            P(None, None, "x"),
            P(None, "x"),
            P(None, "x"),
            P(None, "x"),
            P(None, "x", SP),
        ),
        out_specs=P(SP, "x"),
        check_vma=False,
    )
```

```python
import functools

import jax
import jax.numpy as jnp
from jax import lax
from jax.experimental import pallas as pl
from jax.experimental.pallas import tpu as pltpu
from jax.sharding import Mesh
from jax.sharding import PartitionSpec as P


SP = ("z", "y", "c")
EDGE = 16
LANES = 128
norm_floor = 0.01
bf16, f32 = jnp.bfloat16, jnp.float32


def to_all(array, axis):
    copies = jnp.broadcast_to(array, (lax.axis_size(axis), *array.shape))
    return lax.all_to_all(copies, axis, split_axis=0, concat_axis=0, tiled=True)


def shifted(array, axis, s):
    n = lax.axis_size(axis)
    return lax.ppermute(array, axis, [(i, (i + s) % n) for i in range(n)])


def spread(array, axis):
    n = lax.axis_size(axis)
    pieces = {s: shifted(array, axis, s) for s in (n // 2, 1, n - 1)}
    return [array] + [pieces[s] for s in range(1, n)]


def swap(arrays):
    return [shifted(a, "c", 1) for a in arrays]


def after(arrays, *others):
    return lax.optimization_barrier((tuple(arrays), *others))[0]


def behind(position, s, n):
    return lax.rem(position + (n - s), n)


def by_rows(rows, work, step=64):
    def one(i, carry):
        work(pl.multiple_of(i * step, step), step)
        return carry

    lax.fori_loop(0, rows // step, one, 0)
    if rows % step:
        work(rows - rows % step, rows % step)


def up_kernel(layer, total, n_s, n_y, first_lane, info, *refs):
    streams, refs = refs[:n_s], refs[n_s:]
    gain, tap_ref, bias, ln_gain, ln_shift, refs = *refs[:5], refs[5:]
    pieces, refs = refs[:-7], refs[-7:]
    out, weights, normed, both, padded, columns, sems = refs
    rows, features = normed.shape
    width = streams[0].shape[-1]
    n_x = features // width
    keep = rows - 2 * EDGE
    ch = out.shape[-1]
    outs = [out] if len(out.shape) == 2 else [out.at[b] for b in range(n_x)]
    taps = tap_ref.shape[1]
    shift = EDGE - taps // 2
    core, my_x, my_y = info[0], info[1], info[2]

    if n_y:
        copies = []
        for i, piece in enumerate(pieces if len(pieces) > 2 else [p.at[q] for p in pieces for q in range(n_y)]):
            c = core if i < n_y else 1 - core
            rows_of = weights.at[:, behind(my_y, i % n_y, n_y), c]
            copies.append(pltpu.make_async_copy(piece, rows_of, sems.at[i]))
    else:
        copies = [pltpu.make_async_copy(pieces[0].at[:, pl.ds(first_lane, 2 * ch)], weights, sems.at[0])]
    for copy in copies:
        copy.start()

    def norm(first, step):
        here = pl.ds(first, step)
        squares = jnp.zeros((step, width), f32)
        for s in range(n_x):
            value = (streams[s][here] if n_s > 1 else streams[0][s, here]).astype(f32)
            squares += value * value
        mean = jnp.sum(squares, axis=-1, keepdims=True) * (1.0 / features)
        scale = lax.rsqrt(mean + norm_floor)
        for s in range(n_x):
            b = behind(my_x, s, n_x) if n_s > 1 else s
            wide = pl.ds(pl.multiple_of(b * width, width), width)
            value = (streams[s][here] if n_s > 1 else streams[0][s, here]).astype(f32)
            normed[here, wide] = (value * scale * gain[layer : layer + 1, wide]).astype(bf16)

    by_rows(rows, norm)
    for copy in copies:
        copy.wait()
    for half in range(2):
        part = weights[..., half * ch : (half + 1) * ch].reshape(features, ch)
        both[half] = jnp.dot(normed[...], part, preferred_element_type=f32)

    def gate(first, step):
        here = pl.ds(first, step)
        gated = both[0, here] * jax.nn.sigmoid(both[1, here])
        t = info[3 + layer] + first + lax.broadcasted_iota(jnp.int32, (step, 1), 0)
        gated = jnp.where((t >= 0) & (t < total), gated, 0.0).astype(bf16)
        padded[here] = gated.astype(f32)

    by_rows(rows, gate)
    columns[pl.ds(keep, 2 * ch - keep)] = jnp.zeros((2 * ch - keep, LANES), f32)

    def filtered(first, size):
        window = size + 2 * EDGE
        accs = []
        for start in range(0, ch, LANES):
            lanes = slice(start, start + LANES)
            win = padded[pl.ds(first, window), lanes]
            acc = jnp.zeros((size, LANES), f32) + bias[layer : layer + 1, lanes]
            for r in range(8):
                turned = pltpu.roll(win, window - r, 0) if r else win
                for q in range(window // 8):
                    k = 8 * q + r - shift
                    if 0 <= k < taps:
                        acc = acc + tap_ref[layer, k : k + 1, lanes] * turned[8 * q : 8 * q + size]
            accs.append(acc)
        mean = jnp.sum(sum(accs), axis=-1, keepdims=True) * (1.0 / ch)
        for start, acc in zip(range(0, ch, LANES), accs):
            for to in outs:
                to[pl.ds(first, size), start : start + LANES] = (acc - mean).astype(bf16)
        high = mean.astype(bf16).astype(f32)
        lane = lax.broadcasted_iota(jnp.int32, (size, LANES), 1)
        columns[pl.ds(first, size)] = jnp.where(lane == 0, high, jnp.where(lane == 1, mean - high, 0.0))

    by_rows(keep, filtered)
    across = columns[...].T[:8]
    params = jnp.concatenate([ln_gain[layer : layer + 1, :], ln_shift[layer : layer + 1, :]], axis=1)
    row = lax.broadcasted_iota(jnp.int32, across.shape, 0)
    for p in range(3):
        part = params.astype(bf16).astype(f32)
        across = jnp.where(row == 2 + p, part, across)
        params = params - part
    tail = jnp.concatenate([across[:, :ch], across[:, ch:]], axis=0).astype(bf16)
    for to in outs:
        to[keep:] = tail


def down_kernel(last, n_s, n_y, n_x, n_g, first_lane, info, *refs):
    gated, refs = refs[:n_g], refs[n_g:]
    streams, refs = refs[:n_s], refs[n_s:]
    pieces, refs = refs[:-5], refs[-5:]
    out, weights, act, columns, sems = refs
    core, my_x, my_y = info[0], info[1], info[2]
    if n_g == 1:
        gated = [gated[0].at[behind(my_x, s, n_x)] for s in range(n_x)]
    rows, ch = gated[0].shape
    keep = rows - EDGE
    width = out.shape[-1]

    copies = []

    def fetch(source, to):
        copies.append(pltpu.make_async_copy(source, to, sems.at[len(copies)]))

    if n_y:
        for i, piece in enumerate(pieces):
            c = core if i < n_y else 1 - core
            fetch(piece, weights.at[:, behind(my_y, i % n_y, n_y), c])
    elif last:
        mine = pl.ds(pl.multiple_of(my_x * width, width), width)
        fetch(pieces[0].at[mine, pl.ds(first_lane, ch)], weights.at[:, pl.ds(0, ch)])
        for s in range(1, n_x):
            fetch(pieces[s], weights.at[:, pl.ds(s * ch, ch)])
    else:
        fetch(pieces[0].at[:, pl.ds(first_lane, n_x * ch)], weights)
    for copy in copies:
        copy.start()

    spans = []
    for s in range(n_x):
        tail = gated[s][keep:].astype(f32)
        spans.append(jnp.concatenate([tail[:8], tail[8:]], axis=1))
    params = [sum(v[2 + p : 3 + p] for p in range(3)) for v in spans]
    spans.append(jnp.zeros((LANES - 8 * n_x, 2 * ch), f32))
    columns[...] = jnp.concatenate(spans, axis=0).T

    def activate(first, size):
        here = pl.ds(first, size)
        cols = columns[here]
        means = [cols[:, 8 * s : 8 * s + 1] + cols[:, 8 * s + 1 : 8 * s + 2] for s in range(n_x)]
        average = sum(means) * (1.0 / n_x)
        squares = jnp.zeros((size, ch), f32)
        for s in range(n_x):
            value = gated[s][here].astype(f32) + (means[s] - average)
            squares += value * value
        mean = jnp.sum(squares, axis=-1, keepdims=True) * (1.0 / (n_x * ch))
        scale = lax.rsqrt(mean + norm_floor)
        for s in range(n_x):
            value = (gated[s][here].astype(f32) + (means[s] - average)) * scale
            value = value * params[s][:, :ch] + params[s][:, ch:]
            act[here, s * ch : (s + 1) * ch] = (value * jax.nn.sigmoid(value)).astype(bf16)

    by_rows(keep, activate)
    for copy in copies:
        copy.wait()
    dims = (((1,), (1,)), ((), ()))
    inner = slice(EDGE, EDGE + keep)
    if last:
        added = lax.dot_general(act[...], weights[...], dims, preferred_element_type=f32)
        out[...] = (streams[0][my_x, inner].astype(f32) + added).astype(bf16)
    else:
        part_rows = weights.shape[0] // n_x

        def block(b, base):
            part = weights[pl.ds(b * part_rows, part_rows)].reshape(width, n_x * ch)
            added = lax.dot_general(act[...], part, dims, preferred_element_type=f32)
            out[b] = (base.astype(f32) + added).astype(bf16)

        if n_s > 1:
            for s in range(n_x):
                block(behind(my_x, s, n_x), streams[s][inner])
        else:
            lax.fori_loop(0, n_x, lambda b, carry: (block(b, streams[0][b, inner]), carry)[1], 0)


def vmem():
    return pl.BlockSpec(memory_space=pltpu.VMEM)


def hbm():
    return pl.BlockSpec(memory_space=pltpu.HBM)


def smem():
    return pl.BlockSpec(memory_space=pltpu.SMEM)


def up(layer, total, info, streams, params, pieces, ch, fan, first_lane=0):
    rows, width = streams[0].shape[-2:]
    n_x = params[0].shape[1] // width
    keep = rows - 2 * EDGE
    n_y, shape = 0, (n_x * width,)
    if len(pieces) > 1:
        n_z, n_i, _ = pieces[0].shape[-3:]
        n_y = pieces[0].shape[0] if len(pieces) == 2 else len(pieces) // 2
        shape = (n_z, n_y, 2, n_i)
    return pl.pallas_call(
        functools.partial(up_kernel, layer, total, len(streams), n_y, first_lane),
        out_shape=jax.ShapeDtypeStruct((n_x, keep + EDGE, ch) if fan else (keep + EDGE, ch), bf16),
        in_specs=[smem()] + [vmem()] * (len(streams) + len(params)) + [hbm()] * len(pieces),
        out_specs=vmem(),
        scratch_shapes=[
            pltpu.VMEM((*shape, 2 * ch), bf16),
            pltpu.VMEM((rows, n_x * width), bf16),
            pltpu.VMEM((2, rows, ch), f32),
            pltpu.VMEM((rows, ch), f32),
            pltpu.VMEM((2 * ch, LANES), f32),
            pltpu.SemaphoreType.DMA((max(1, 2 * n_y),)),
        ],
    )(info, *streams, *params, *pieces)


def down(last, info, gated, streams, pieces, paired, first_lane=0):
    rows, ch = gated[0].shape[-2:]
    n_x = lax.axis_size("x")
    keep = rows - EDGE
    width = streams[0].shape[-1]
    n_y = len(pieces) // 2 if paired else 0
    shape = (width if last else n_x * width,)
    if paired:
        n_z, n_i, _ = pieces[0].shape
        shape = (n_z, n_y, 2, n_i)
    out_shape = (keep, width) if last else (n_x, keep, width)
    return pl.pallas_call(
        functools.partial(down_kernel, last, len(streams), n_y, n_x, len(gated), first_lane),
        out_shape=jax.ShapeDtypeStruct(out_shape, bf16),
        in_specs=[smem()] + [vmem()] * (len(gated) + len(streams)) + [hbm()] * len(pieces),
        out_specs=vmem(),
        scratch_shapes=[
            pltpu.VMEM((*shape, n_x * ch), bf16),
            pltpu.VMEM((keep, n_x * ch), bf16),
            pltpu.VMEM((2 * ch, LANES), f32),
            pltpu.SemaphoreType.DMA((len(pieces),)),
        ],
    )(info, *gated, *streams, *pieces)


def program(tokens, norm_gain, w_value, w_gate, conv_taps, conv_bias, ln_gain, ln_shift, w_out):
    layers, _, ch = w_value.shape
    n_x = lax.axis_size("x")
    my_x = lax.axis_index("x")
    n_tok, f_loc = tokens.shape
    halo = EDGE * layers
    size = lax.axis_size(SP)
    total = size * n_tok
    place = lax.axis_index(SP) * n_tok
    info = jnp.stack(
        [lax.axis_index("c"), my_x, lax.axis_index("y")]
        + [place - EDGE * (layers - l) for l in range(layers)]
    ).astype(jnp.int32)
    params = (norm_gain, conv_taps, conv_bias, ln_gain, ln_shift)

    def gather_z(array):
        return to_all(array, "z")

    near = 2
    ups = [gather_z(jnp.concatenate([w_value[l], w_gate[l]], axis=1)) for l in range(near)]

    out_t = jnp.swapaxes(w_out, 1, 2)
    wide = jnp.concatenate(spread(out_t[: layers - 1], "x"), axis=-1)

    packs, lanes, at = [], [(0, 0)], 0
    for l in range(1, layers):
        pair = [w_value[l], w_gate[l]] if l >= near else []
        packs += [*pair, out_t[l] if l == layers - 1 else wide[l]]
        lanes.append((at, at + sum(a.shape[1] for a in pair)))
        at = lanes[-1][1] + packs[-1].shape[1]
    rest = lax.all_gather(jnp.concatenate(packs, axis=1), SP, axis=0, tiled=True)

    before = lax.ppermute(tokens[n_tok - halo :], SP, [(i, i + 1) for i in range(size - 1)])
    following = lax.ppermute(tokens[:halo], SP, [(i + 1, i) for i in range(size - 1)])
    streams = spread(jnp.concatenate([before, tokens, following], axis=0), "x")

    ups = [spread(a, "y") for a in ups]
    out_first = spread(gather_z(wide[0]), "y")

    for l in range(layers):
        last = l == layers - 1
        first, start = lanes[l]
        pieces = [rest]
        if l < near:
            pieces = [jnp.stack(after(ups[l], stream))] if l else ups[l]
            pieces = [*pieces, *swap(pieces)]
        gated = up(l, total, info, streams, params, pieces, ch, l > 0, first)
        if l:
            gated = [lax.all_to_all(gated, "x", split_axis=0, concat_axis=0, tiled=True)]
        else:
            gated = spread(gated, "x")
        pieces = [rest]
        if l == 0:
            pieces = after(out_first, *gated[1:])
            pieces = [*pieces, *swap(pieces)]
        if last:
            for s in (1, n_x // 2, n_x - 1):
                row = lax.rem(my_x + s, n_x) * f_loc
                block = lax.dynamic_slice(rest, (row, start), (f_loc, ch))
                pieces.append(shifted(block, "x", s))
        stream = down(last, info, gated, streams, pieces, l == 0, start)
        streams = [stream]
    return stream


def solution(mesh):
    torus = Mesh(mesh.devices.reshape(8, 4, 2, mesh.shape["tp"]), ("z", "y", "c", "x"))
    return jax.shard_map(
        program,
        mesh=torus,
        in_specs=(
            P(SP, "x"),
            P(),
            P(None, SP, "x"),
            P(None, SP, "x"),
            P(None, None, "x"),
            P(None, "x"),
            P(None, "x"),
            P(None, "x"),
            P(None, "x", SP),
        ),
        out_specs=P(SP, "x"),
        check_vma=False,
    )
```

```python
import functools

import jax
import jax.numpy as jnp
from jax import lax
from jax.experimental import pallas as pl
from jax.experimental.pallas import tpu as pltpu
from jax.sharding import Mesh
from jax.sharding import PartitionSpec as P


SP = ("z", "y", "c")
EDGE = 16
LANES = 128
norm_floor = 0.01
bf16, f32 = jnp.bfloat16, jnp.float32


def to_all(array, axis):
    copies = jnp.broadcast_to(array, (lax.axis_size(axis), *array.shape))
    return lax.all_to_all(copies, axis, split_axis=0, concat_axis=0, tiled=True)


def shifted(array, axis, s):
    n = lax.axis_size(axis)
    return lax.ppermute(array, axis, [(i, (i + s) % n) for i in range(n)])


def spread(array, axis):
    n = lax.axis_size(axis)
    pieces = {s: shifted(array, axis, s) for s in (n // 2, 1, n - 1)}
    return [array] + [pieces[s] for s in range(1, n)]


def swap(arrays):
    return [shifted(a, "c", 1) for a in arrays]


def after(arrays, *others):
    return lax.optimization_barrier((tuple(arrays), *others))[0]


def behind(position, s, n):
    return lax.rem(position + (n - s), n)


def by_rows(rows, work, step=64):
    def one(i, carry):
        work(pl.multiple_of(i * step, step), step)
        return carry

    lax.fori_loop(0, rows // step, one, 0)
    if rows % step:
        work(rows - rows % step, rows % step)


def up_kernel(layer, total, n_s, n_y, first_lane, info, *refs):
    streams, refs = refs[:n_s], refs[n_s:]
    gain, tap_ref, bias, ln_gain, ln_shift, refs = *refs[:5], refs[5:]
    pieces, refs = refs[:-8], refs[-8:]
    out, weights, normed, scales, both, padded, columns, sems = refs
    rows, features = normed.shape
    width = streams[0].shape[-1]
    n_x = features // width
    keep = rows - 2 * EDGE
    ch = out.shape[-1]
    outs = [out] if len(out.shape) == 2 else [out.at[b] for b in range(n_x)]
    taps = tap_ref.shape[1]
    shift = EDGE - taps // 2
    core, my_x, my_y = info[0], info[1], info[2]

    if n_y:
        copies = []
        for i, piece in enumerate(pieces):
            c = core if i < n_y else 1 - core
            rows_of = weights.at[:, behind(my_y, i % n_y, n_y), c]
            copies.append(pltpu.make_async_copy(piece.at[:, :, pl.ds(first_lane, 2 * ch)], rows_of, sems.at[i]))
    else:
        copies = [pltpu.make_async_copy(pieces[0].at[:, pl.ds(first_lane, 2 * ch)], weights, sems.at[0])]
    for copy in copies:
        copy.start()

    def norm(first, step):
        here = pl.ds(first, step)
        squares = jnp.zeros((step, width), f32)
        for s in range(n_x):
            b = behind(my_x, s, n_x) if n_s > 1 else s
            wide = pl.ds(pl.multiple_of(b * width, width), width)
            value = (streams[s][here] if n_s > 1 else streams[0][s, here]).astype(f32)
            squares += value * value
            normed[here, wide] = (value * gain[layer : layer + 1, wide]).astype(bf16)
        mean = jnp.sum(squares, axis=-1, keepdims=True) * (1.0 / features)
        scales[here] = jnp.broadcast_to(lax.rsqrt(mean + norm_floor), (step, LANES))

    by_rows(rows, norm)
    for copy in copies:
        copy.wait()
    for half in range(2):
        part = weights[..., half * ch : (half + 1) * ch].reshape(features, ch)
        both[half] = jnp.dot(normed[...], part, preferred_element_type=f32)

    def gate(first, step):
        here = pl.ds(first, step)
        scale = scales[here, 0:1]
        gated = both[0, here] * scale * jax.nn.sigmoid(both[1, here] * scale)
        t = info[3 + layer] + first + lax.broadcasted_iota(jnp.int32, (step, 1), 0)
        gated = jnp.where((t >= 0) & (t < total), gated, 0.0).astype(bf16)
        padded[here] = gated.astype(f32)

    by_rows(rows, gate)
    columns[pl.ds(keep, 2 * ch - keep)] = jnp.zeros((2 * ch - keep, LANES), f32)

    def filtered(first, size):
        window = size + 2 * EDGE
        accs = []
        for start in range(0, ch, LANES):
            lanes = slice(start, start + LANES)
            win = padded[pl.ds(first, window), lanes]
            acc = jnp.zeros((size, LANES), f32) + bias[layer : layer + 1, lanes]
            for r in range(8):
                turned = pltpu.roll(win, window - r, 0) if r else win
                for q in range(window // 8):
                    k = 8 * q + r - shift
                    if 0 <= k < taps:
                        acc = acc + tap_ref[layer, k : k + 1, lanes] * turned[8 * q : 8 * q + size]
            accs.append(acc)
        mean = jnp.sum(sum(accs), axis=-1, keepdims=True) * (1.0 / ch)
        for start, acc in zip(range(0, ch, LANES), accs):
            for to in outs:
                to[pl.ds(first, size), start : start + LANES] = (acc - mean).astype(bf16)
        high = mean.astype(bf16).astype(f32)
        lane = lax.broadcasted_iota(jnp.int32, (size, LANES), 1)
        columns[pl.ds(first, size)] = jnp.where(lane == 0, high, jnp.where(lane == 1, mean - high, 0.0))

    by_rows(keep, filtered)
    across = columns[...].T[:8]
    params = jnp.concatenate([ln_gain[layer : layer + 1, :], ln_shift[layer : layer + 1, :]], axis=1)
    row = lax.broadcasted_iota(jnp.int32, across.shape, 0)
    for p in range(3):
        part = params.astype(bf16).astype(f32)
        across = jnp.where(row == 2 + p, part, across)
        params = params - part
    tail = jnp.concatenate([across[:, :ch], across[:, ch:]], axis=0).astype(bf16)
    for to in outs:
        to[keep:] = tail


def down_kernel(last, n_s, n_y, n_x, n_g, first_lane, info, *refs):
    gated, refs = refs[:n_g], refs[n_g:]
    streams, refs = refs[:n_s], refs[n_s:]
    pieces, refs = refs[:-5], refs[-5:]
    out, weights, act, columns, sems = refs
    core, my_x, my_y = info[0], info[1], info[2]
    if n_g == 1:
        gated = [gated[0].at[behind(my_x, s, n_x)] for s in range(n_x)]
    rows, ch = gated[0].shape
    keep = rows - EDGE
    width = out.shape[-1]

    copies = []

    def fetch(source, to):
        copies.append(pltpu.make_async_copy(source, to, sems.at[len(copies)]))

    if n_y:
        for i, piece in enumerate(pieces):
            c = core if i < n_y else 1 - core
            fetch(piece, weights.at[:, behind(my_y, i % n_y, n_y), c])
    elif last:
        mine = pl.ds(pl.multiple_of(my_x * width, width), width)
        fetch(pieces[0].at[mine, pl.ds(first_lane, n_x * ch)], weights)
    else:
        fetch(pieces[0].at[:, pl.ds(first_lane, n_x * ch)], weights)
    for copy in copies:
        copy.start()

    spans = []
    for s in range(n_x):
        tail = gated[s][keep:].astype(f32)
        spans.append(jnp.concatenate([tail[:8], tail[8:]], axis=1))
    params = [sum(v[2 + p : 3 + p] for p in range(3)) for v in spans]
    spans.append(jnp.zeros((LANES - 8 * n_x, 2 * ch), f32))
    columns[...] = jnp.concatenate(spans, axis=0).T

    def activate(first, size):
        here = pl.ds(first, size)
        cols = columns[here]
        means = [cols[:, 8 * s : 8 * s + 1] + cols[:, 8 * s + 1 : 8 * s + 2] for s in range(n_x)]
        average = sum(means) * (1.0 / n_x)
        squares = jnp.zeros((size, ch), f32)
        for s in range(n_x):
            value = gated[s][here].astype(f32) + (means[s] - average)
            squares += value * value
        mean = jnp.sum(squares, axis=-1, keepdims=True) * (1.0 / (n_x * ch))
        scale = lax.rsqrt(mean + norm_floor)
        for s in range(n_x):
            value = (gated[s][here].astype(f32) + (means[s] - average)) * scale
            value = value * params[s][:, :ch] + params[s][:, ch:]
            act[here, s * ch : (s + 1) * ch] = (value * jax.nn.sigmoid(value)).astype(bf16)

    by_rows(keep, activate)
    for copy in copies:
        copy.wait()
    dims = (((1,), (1,)), ((), ()))
    inner = slice(EDGE, EDGE + keep)
    if last:
        added = lax.dot_general(act[...], weights[...], dims, preferred_element_type=f32)
        out[...] = (streams[0][my_x, inner].astype(f32) + added).astype(bf16)
    else:
        part_rows = weights.shape[0] // n_x

        def block(b, base):
            part = weights[pl.ds(b * part_rows, part_rows)].reshape(width, n_x * ch)
            added = lax.dot_general(act[...], part, dims, preferred_element_type=f32)
            out[b] = (base.astype(f32) + added).astype(bf16)

        if n_s > 1:
            for s in range(n_x):
                block(behind(my_x, s, n_x), streams[s][inner])
        else:
            lax.fori_loop(0, n_x, lambda b, carry: (block(b, streams[0][b, inner]), carry)[1], 0)


def vmem():
    return pl.BlockSpec(memory_space=pltpu.VMEM)


def hbm():
    return pl.BlockSpec(memory_space=pltpu.HBM)


def smem():
    return pl.BlockSpec(memory_space=pltpu.SMEM)


def up(layer, total, info, streams, params, pieces, ch, fan, first_lane=0):
    rows, width = streams[0].shape[-2:]
    n_x = params[0].shape[1] // width
    keep = rows - 2 * EDGE
    n_y, shape = 0, (n_x * width,)
    if len(pieces) > 1:
        n_z, n_i, _ = pieces[0].shape[-3:]
        n_y = len(pieces) // 2
        shape = (n_z, n_y, 2, n_i)
    return pl.pallas_call(
        functools.partial(up_kernel, layer, total, len(streams), n_y, first_lane),
        out_shape=jax.ShapeDtypeStruct((n_x, keep + EDGE, ch) if fan else (keep + EDGE, ch), bf16),
        in_specs=[smem()] + [vmem()] * (len(streams) + len(params)) + [hbm()] * len(pieces),
        out_specs=vmem(),
        scratch_shapes=[
            pltpu.VMEM((*shape, 2 * ch), bf16),
            pltpu.VMEM((rows, n_x * width), bf16),
            pltpu.VMEM((rows, LANES), f32),
            pltpu.VMEM((2, rows, ch), f32),
            pltpu.VMEM((rows, ch), f32),
            pltpu.VMEM((2 * ch, LANES), f32),
            pltpu.SemaphoreType.DMA((max(1, 2 * n_y),)),
        ],
    )(info, *streams, *params, *pieces)


def down(last, info, gated, streams, pieces, paired, first_lane=0):
    rows, ch = gated[0].shape[-2:]
    n_x = lax.axis_size("x")
    keep = rows - EDGE
    width = streams[0].shape[-1]
    n_y = len(pieces) // 2 if paired else 0
    shape = (width if last else n_x * width,)
    if paired:
        n_z, n_i, _ = pieces[0].shape
        shape = (n_z, n_y, 2, n_i)
    out_shape = (keep, width) if last else (n_x, keep, width)
    return pl.pallas_call(
        functools.partial(down_kernel, last, len(streams), n_y, n_x, len(gated), first_lane),
        out_shape=jax.ShapeDtypeStruct(out_shape, bf16),
        in_specs=[smem()] + [vmem()] * (len(gated) + len(streams)) + [hbm()] * len(pieces),
        out_specs=vmem(),
        scratch_shapes=[
            pltpu.VMEM((*shape, n_x * ch), bf16),
            pltpu.VMEM((keep, n_x * ch), bf16),
            pltpu.VMEM((2 * ch, LANES), f32),
            pltpu.SemaphoreType.DMA((len(pieces),)),
        ],
    )(info, *gated, *streams, *pieces)


def program(tokens, norm_gain, w_value, w_gate, conv_taps, conv_bias, ln_gain, ln_shift, w_out):
    layers, _, ch = w_value.shape
    n_x = lax.axis_size("x")
    my_x = lax.axis_index("x")
    n_tok, _ = tokens.shape
    halo = EDGE * layers
    size = lax.axis_size(SP)
    total = size * n_tok
    place = lax.axis_index(SP) * n_tok
    info = jnp.stack(
        [lax.axis_index("c"), my_x, lax.axis_index("y")]
        + [place - EDGE * (layers - l) for l in range(layers)]
    ).astype(jnp.int32)
    params = (norm_gain, conv_taps, conv_bias, ln_gain, ln_shift)

    def gather_z(array):
        return to_all(array, "z")

    near = min(2, layers)
    pairs = [w for l in range(near) for w in (w_value[l], w_gate[l])]
    ups = gather_z(jnp.concatenate(pairs, axis=1))

    wide = jnp.concatenate(spread(jnp.swapaxes(w_out, 1, 2), "x"), axis=-1)

    packs, lanes, at = [], [(0, 0)], 0
    for l in range(1, layers):
        pair = [w_value[l], w_gate[l]] if l >= near else []
        packs += [*pair, wide[l]]
        first = at if pair else 2 * ch * l
        lanes.append((first, at + 2 * ch * bool(pair)))
        at = lanes[-1][1] + n_x * ch
    rest = lax.all_gather(jnp.concatenate(packs, axis=1), SP, axis=0, tiled=True)

    before = lax.ppermute(tokens[n_tok - halo :], SP, [(i, i + 1) for i in range(size - 1)])
    following = lax.ppermute(tokens[:halo], SP, [(i + 1, i) for i in range(size - 1)])
    streams = spread(jnp.concatenate([before, tokens, following], axis=0), "x")

    ups = spread(ups, "y")
    outs = spread(gather_z(wide[0]), "y")
    ups = [*ups, *swap(ups)]

    for l in range(layers):
        first, start = lanes[l]
        gated = up(l, total, info, streams, params, ups if l < near else [rest], ch, True, first)
        gated = lax.all_to_all(gated, "x", split_axis=0, concat_axis=0, tiled=True)
        pieces = [rest]
        if l == 0:
            pieces = after(outs, gated)
            pieces = [*pieces, *swap(pieces)]
        stream = down(l == layers - 1, info, [gated], streams, pieces, l == 0, start)
        streams = [stream]
    return stream


def solution(mesh):
    torus = Mesh(mesh.devices.reshape(8, 4, 2, mesh.shape["tp"]), ("z", "y", "c", "x"))
    return jax.shard_map(
        program,
        mesh=torus,
        in_specs=(
            P(SP, "x"),
            P(),
            P(None, SP, "x"),
            P(None, SP, "x"),
            P(None, None, "x"),
            P(None, "x"),
            P(None, "x"),
            P(None, "x"),
            P(None, "x", SP),
        ),
        out_specs=P(SP, "x"),
        check_vma=False,
    )
```

```python
import functools

import jax
import jax.numpy as jnp
from jax import lax
from jax.experimental import pallas as pl
from jax.experimental.pallas import tpu as pltpu
from jax.sharding import Mesh
from jax.sharding import PartitionSpec as P


SP = ("z", "y", "c")
EDGE = 16
LANES = 128
norm_floor = 0.01
bf16, f32 = jnp.bfloat16, jnp.float32


def to_all(array, axis):
    copies = jnp.broadcast_to(array, (lax.axis_size(axis), *array.shape))
    return lax.all_to_all(copies, axis, split_axis=0, concat_axis=0, tiled=True)


def shifted(array, axis, s):
    n = lax.axis_size(axis)
    return lax.ppermute(array, axis, [(i, (i + s) % n) for i in range(n)])


def spread(array, axis):
    n = lax.axis_size(axis)
    pieces = {s: shifted(array, axis, s) for s in (n // 2, 1, n - 1)}
    return [array] + [pieces[s] for s in range(1, n)]


def swap(arrays):
    return [shifted(a, "c", 1) for a in arrays]


def after(arrays, *others):
    return lax.optimization_barrier((tuple(arrays), *others))[0]


def behind(position, s, n):
    return lax.rem(position + (n - s), n)


def by_rows(rows, work, step=64):
    def one(i, carry):
        work(pl.multiple_of(i * step, step), step)
        return carry

    lax.fori_loop(0, rows // step, one, 0)
    if rows % step:
        work(rows - rows % step, rows % step)


def up_kernel(layer, total, n_s, n_y, first_lane, info, *refs):
    streams, refs = refs[:n_s], refs[n_s:]
    gain, tap_ref, bias, ln_gain, ln_shift, refs = *refs[:5], refs[5:]
    pieces, refs = refs[:-7], refs[-7:]
    out, weights, normed, both, padded, columns, sems = refs
    rows, features = normed.shape
    width = streams[0].shape[-1]
    n_x = features // width
    keep = rows - 2 * EDGE
    ch = out.shape[-1]
    outs = [out] if len(out.shape) == 2 else [out.at[b] for b in range(n_x)]
    taps = tap_ref.shape[1]
    shift = EDGE - taps // 2
    core, my_x, my_y = info[0], info[1], info[2]

    if n_y:
        copies = []
        for i, piece in enumerate(pieces):
            c = core if i < n_y else 1 - core
            rows_of = weights.at[:, behind(my_y, i % n_y, n_y), c]
            copies.append(pltpu.make_async_copy(piece.at[:, :, pl.ds(first_lane, 2 * ch)], rows_of, sems.at[i]))
    else:
        copies = [pltpu.make_async_copy(pieces[0].at[:, pl.ds(first_lane, 2 * ch)], weights, sems.at[0])]
    for copy in copies:
        copy.start()

    def norm(first, step):
        here = pl.ds(first, step)
        squares = jnp.zeros((step, width), f32)
        for s in range(n_x):
            value = (streams[s][here] if n_s > 1 else streams[0][s, here]).astype(f32)
            squares += value * value
        mean = jnp.sum(squares, axis=-1, keepdims=True) * (1.0 / features)
        scale = lax.rsqrt(mean + norm_floor)
        for s in range(n_x):
            b = behind(my_x, s, n_x) if n_s > 1 else s
            wide = pl.ds(pl.multiple_of(b * width, width), width)
            value = (streams[s][here] if n_s > 1 else streams[0][s, here]).astype(f32)
            normed[here, wide] = (value * scale * gain[layer : layer + 1, wide]).astype(bf16)

    by_rows(rows, norm)
    for copy in copies:
        copy.wait()
    for half in range(2):
        part = weights[..., half * ch : (half + 1) * ch].reshape(features, ch)
        both[half] = jnp.dot(normed[...], part, preferred_element_type=f32)

    def gate(first, step):
        here = pl.ds(first, step)
        gated = both[0, here] * jax.nn.sigmoid(both[1, here])
        t = info[3 + layer] + first + lax.broadcasted_iota(jnp.int32, (step, 1), 0)
        gated = jnp.where((t >= 0) & (t < total), gated, 0.0).astype(bf16)
        padded[here] = gated.astype(f32)

    by_rows(rows, gate)
    columns[pl.ds(keep, 2 * ch - keep)] = jnp.zeros((2 * ch - keep, LANES), f32)

    def filtered(first, size):
        window = size + 2 * EDGE
        accs = []
        for start in range(0, ch, LANES):
            lanes = slice(start, start + LANES)
            win = padded[pl.ds(first, window), lanes]
            acc = jnp.zeros((size, LANES), f32) + bias[layer : layer + 1, lanes]
            for r in range(8):
                turned = pltpu.roll(win, window - r, 0) if r else win
                for q in range(window // 8):
                    k = 8 * q + r - shift
                    if 0 <= k < taps:
                        acc = acc + tap_ref[layer, k : k + 1, lanes] * turned[8 * q : 8 * q + size]
            accs.append(acc)
        mean = jnp.sum(sum(accs), axis=-1, keepdims=True) * (1.0 / ch)
        for start, acc in zip(range(0, ch, LANES), accs):
            for to in outs:
                to[pl.ds(first, size), start : start + LANES] = (acc - mean).astype(bf16)
        high = mean.astype(bf16).astype(f32)
        lane = lax.broadcasted_iota(jnp.int32, (size, LANES), 1)
        columns[pl.ds(first, size)] = jnp.where(lane == 0, high, jnp.where(lane == 1, mean - high, 0.0))

    by_rows(keep, filtered)
    across = columns[...].T[:8]
    params = jnp.concatenate([ln_gain[layer : layer + 1, :], ln_shift[layer : layer + 1, :]], axis=1)
    row = lax.broadcasted_iota(jnp.int32, across.shape, 0)
    for p in range(3):
        part = params.astype(bf16).astype(f32)
        across = jnp.where(row == 2 + p, part, across)
        params = params - part
    tail = jnp.concatenate([across[:, :ch], across[:, ch:]], axis=0).astype(bf16)
    for to in outs:
        to[keep:] = tail


def down_kernel(last, n_s, n_y, n_x, n_g, first_lane, info, *refs):
    gated, refs = refs[:n_g], refs[n_g:]
    streams, refs = refs[:n_s], refs[n_s:]
    pieces, refs = refs[:-5], refs[-5:]
    out, weights, act, columns, sems = refs
    core, my_x, my_y = info[0], info[1], info[2]
    if n_g == 1:
        gated = [gated[0].at[behind(my_x, s, n_x)] for s in range(n_x)]
    rows, ch = gated[0].shape
    keep = rows - EDGE
    width = out.shape[-1]

    copies = []

    def fetch(source, to):
        copies.append(pltpu.make_async_copy(source, to, sems.at[len(copies)]))

    if n_y:
        for i, piece in enumerate(pieces):
            c = core if i < n_y else 1 - core
            fetch(piece, weights.at[:, behind(my_y, i % n_y, n_y), c])
    elif last:
        mine = pl.ds(pl.multiple_of(my_x * width, width), width)
        fetch(pieces[0].at[mine, pl.ds(first_lane, n_x * ch)], weights)
    else:
        fetch(pieces[0].at[:, pl.ds(first_lane, n_x * ch)], weights)
    for copy in copies:
        copy.start()

    spans = []
    for s in range(n_x):
        tail = gated[s][keep:].astype(f32)
        spans.append(jnp.concatenate([tail[:8], tail[8:]], axis=1))
    params = [sum(v[2 + p : 3 + p] for p in range(3)) for v in spans]
    spans.append(jnp.zeros((LANES - 8 * n_x, 2 * ch), f32))
    columns[...] = jnp.concatenate(spans, axis=0).T

    def activate(first, size):
        here = pl.ds(first, size)
        cols = columns[here]
        means = [cols[:, 8 * s : 8 * s + 1] + cols[:, 8 * s + 1 : 8 * s + 2] for s in range(n_x)]
        average = sum(means) * (1.0 / n_x)
        squares = jnp.zeros((size, ch), f32)
        for s in range(n_x):
            value = gated[s][here].astype(f32) + (means[s] - average)
            squares += value * value
        mean = jnp.sum(squares, axis=-1, keepdims=True) * (1.0 / (n_x * ch))
        scale = lax.rsqrt(mean + norm_floor)
        for s in range(n_x):
            value = (gated[s][here].astype(f32) + (means[s] - average)) * scale
            value = value * params[s][:, :ch] + params[s][:, ch:]
            act[here, s * ch : (s + 1) * ch] = (value * jax.nn.sigmoid(value)).astype(bf16)

    by_rows(keep, activate)
    for copy in copies:
        copy.wait()
    dims = (((1,), (1,)), ((), ()))
    inner = slice(EDGE, EDGE + keep)
    if last:
        added = lax.dot_general(act[...], weights[...], dims, preferred_element_type=f32)
        out[...] = (streams[0][my_x, inner].astype(f32) + added).astype(bf16)
    else:
        part_rows = weights.shape[0] // n_x

        def block(b, base):
            part = weights[pl.ds(b * part_rows, part_rows)].reshape(width, n_x * ch)
            added = lax.dot_general(act[...], part, dims, preferred_element_type=f32)
            out[b] = (base.astype(f32) + added).astype(bf16)

        for s in range(n_x):
            if n_s > 1:
                block(behind(my_x, s, n_x), streams[s][inner])
            else:
                block(s, streams[0][s, inner])


def vmem():
    return pl.BlockSpec(memory_space=pltpu.VMEM)


def hbm():
    return pl.BlockSpec(memory_space=pltpu.HBM)


def smem():
    return pl.BlockSpec(memory_space=pltpu.SMEM)


def up(layer, total, info, streams, params, pieces, ch, fan, first_lane=0):
    rows, width = streams[0].shape[-2:]
    n_x = params[0].shape[1] // width
    keep = rows - 2 * EDGE
    n_y, shape = 0, (n_x * width,)
    if len(pieces) > 1:
        n_z, n_i, _ = pieces[0].shape[-3:]
        n_y = len(pieces) // 2
        shape = (n_z, n_y, 2, n_i)
    return pl.pallas_call(
        functools.partial(up_kernel, layer, total, len(streams), n_y, first_lane),
        out_shape=jax.ShapeDtypeStruct((n_x, keep + EDGE, ch) if fan else (keep + EDGE, ch), bf16),
        in_specs=[smem()] + [vmem()] * (len(streams) + len(params)) + [hbm()] * len(pieces),
        out_specs=vmem(),
        scratch_shapes=[
            pltpu.VMEM((*shape, 2 * ch), bf16),
            pltpu.VMEM((rows, n_x * width), bf16),
            pltpu.VMEM((2, rows, ch), f32),
            pltpu.VMEM((rows, ch), f32),
            pltpu.VMEM((2 * ch, LANES), f32),
            pltpu.SemaphoreType.DMA((max(1, 2 * n_y),)),
        ],
    )(info, *streams, *params, *pieces)


def down(last, info, gated, streams, pieces, paired, first_lane=0):
    rows, ch = gated[0].shape[-2:]
    n_x = lax.axis_size("x")
    keep = rows - EDGE
    width = streams[0].shape[-1]
    n_y = len(pieces) // 2 if paired else 0
    shape = (width if last else n_x * width,)
    if paired:
        n_z, n_i, _ = pieces[0].shape
        shape = (n_z, n_y, 2, n_i)
    out_shape = (keep, width) if last else (n_x, keep, width)
    return pl.pallas_call(
        functools.partial(down_kernel, last, len(streams), n_y, n_x, len(gated), first_lane),
        out_shape=jax.ShapeDtypeStruct(out_shape, bf16),
        in_specs=[smem()] + [vmem()] * (len(gated) + len(streams)) + [hbm()] * len(pieces),
        out_specs=vmem(),
        scratch_shapes=[
            pltpu.VMEM((*shape, n_x * ch), bf16),
            pltpu.VMEM((keep, n_x * ch), bf16),
            pltpu.VMEM((2 * ch, LANES), f32),
            pltpu.SemaphoreType.DMA((len(pieces),)),
        ],
    )(info, *gated, *streams, *pieces)


def program(tokens, norm_gain, w_value, w_gate, conv_taps, conv_bias, ln_gain, ln_shift, w_out):
    layers, _, ch = w_value.shape
    n_x = lax.axis_size("x")
    my_x = lax.axis_index("x")
    n_tok, _ = tokens.shape
    halo = EDGE * layers
    size = lax.axis_size(SP)
    total = size * n_tok
    place = lax.axis_index(SP) * n_tok
    info = jnp.stack(
        [lax.axis_index("c"), my_x, lax.axis_index("y")]
        + [place - EDGE * (layers - l) for l in range(layers)]
    ).astype(jnp.int32)
    params = (norm_gain, conv_taps, conv_bias, ln_gain, ln_shift)

    def gather_z(array):
        return to_all(array, "z")

    near = min(2, layers)
    pairs = [w for l in range(near) for w in (w_value[l], w_gate[l])]
    ups = gather_z(jnp.concatenate(pairs, axis=1))

    wide = jnp.concatenate(spread(jnp.swapaxes(w_out, 1, 2), "x"), axis=-1)

    packs, lanes, at = [], [(0, 0)], 0
    for l in range(1, layers):
        pair = [w_value[l], w_gate[l]] if l >= near else []
        packs += [*pair, wide[l]]
        first = at if pair else 2 * ch * l
        lanes.append((first, at + 2 * ch * bool(pair)))
        at = lanes[-1][1] + n_x * ch
    rest = lax.all_gather(jnp.concatenate(packs, axis=1), SP, axis=0, tiled=True)

    before = lax.ppermute(tokens[n_tok - halo :], SP, [(i, i + 1) for i in range(size - 1)])
    following = lax.ppermute(tokens[:halo], SP, [(i + 1, i) for i in range(size - 1)])
    streams = spread(jnp.concatenate([before, tokens, following], axis=0), "x")

    ups = spread(ups, "y")
    outs = spread(gather_z(wide[0]), "y")
    ups = [*ups, *swap(ups)]

    for l in range(layers):
        first, start = lanes[l]
        gated = up(l, total, info, streams, params, ups if l < near else [rest], ch, True, first)
        gated = lax.all_to_all(gated, "x", split_axis=0, concat_axis=0, tiled=True)
        pieces = [rest]
        if l == 0:
            pieces = after(outs, gated)
            pieces = [*pieces, *swap(pieces)]
        stream = down(l == layers - 1, info, [gated], streams, pieces, l == 0, start)
        streams = [stream]
    return stream


def solution(mesh):
    torus = Mesh(mesh.devices.reshape(8, 4, 2, mesh.shape["tp"]), ("z", "y", "c", "x"))
    return jax.shard_map(
        program,
        mesh=torus,
        in_specs=(
            P(SP, "x"),
            P(),
            P(None, SP, "x"),
            P(None, SP, "x"),
            P(None, None, "x"),
            P(None, "x"),
            P(None, "x"),
            P(None, "x"),
            P(None, "x", SP),
        ),
        out_specs=P(SP, "x"),
        check_vma=False,
    )
```

```python
import functools

import jax
import jax.numpy as jnp
from jax import lax
from jax.experimental import pallas as pl
from jax.experimental.pallas import tpu as pltpu
from jax.sharding import Mesh
from jax.sharding import PartitionSpec as P


SP = ("z", "y", "c")
EDGE = 16
LANES = 128
norm_floor = 0.01
bf16, f32 = jnp.bfloat16, jnp.float32


def to_all(array, axis):
    copies = jnp.broadcast_to(array, (lax.axis_size(axis), *array.shape))
    return lax.all_to_all(copies, axis, split_axis=0, concat_axis=0, tiled=True)


def shifted(array, axis, s):
    n = lax.axis_size(axis)
    return lax.ppermute(array, axis, [(i, (i + s) % n) for i in range(n)])


def spread(array, axis):
    n = lax.axis_size(axis)
    pieces = {s: shifted(array, axis, s) for s in (n // 2, 1, n - 1)}
    return [array] + [pieces[s] for s in range(1, n)]


def swap(arrays):
    return [shifted(a, "c", 1) for a in arrays]


def after(arrays, *others):
    return lax.optimization_barrier((tuple(arrays), *others))[0]


def behind(position, s, n):
    return lax.rem(position + (n - s), n)


def by_rows(rows, work, step=64):
    def one(i, carry):
        work(pl.multiple_of(i * step, step), step)
        return carry

    lax.fori_loop(0, rows // step, one, 0)
    if rows % step:
        work(rows - rows % step, rows % step)


def up_kernel(layer, total, n_s, n_y, first_lane, info, *refs):
    streams, params, refs = refs[:n_s], refs[n_s : n_s + 5], refs[n_s + 5 :]
    pieces, refs = refs[:-7], refs[-7:]
    up_work(layer, total, n_y, first_lane, info, streams, params, pieces, *refs)


def mid_kernel(layer, total, n_s, n_out, down_lane, n_up, up_lane, n_x, info, *refs):
    gated, streams, params, refs = refs[0], refs[1 : 1 + n_s], refs[1 + n_s : 6 + n_s], refs[6 + n_s :]
    split = max(1, 2 * n_out)
    down_pieces, up_pieces, refs = refs[:split], refs[split:-12], refs[-12:]
    stream, out, refs = refs[0], refs[1], refs[2:]
    down_scratch, up_scratch = refs[:4], refs[4:]

    def first():
        down_work(False, n_out, n_x, down_lane, info, gated, streams, down_pieces, stream, *down_scratch)

    up_work(layer + 1, total, n_up, up_lane, info, [stream], params, up_pieces, out, *up_scratch, first=first)


def down_kernel(n_x, first_lane, info, gated, stream, piece, out, *scratch):
    down_work(True, 0, n_x, first_lane, info, gated, [stream], [piece], out, *scratch)


def up_work(
    layer, total, n_y, first_lane, info, streams, params, pieces, out, weights, normed, both, padded, columns, sems, first=None
):
    gain, tap_ref, bias, ln_gain, ln_shift = params
    n_s = len(streams)
    rows, features = normed.shape
    width = streams[0].shape[-1]
    n_x = features // width
    keep = rows - 2 * EDGE
    ch = out.shape[-1]
    outs = [out.at[b] for b in range(n_x)]
    taps = tap_ref.shape[1]
    shift = EDGE - taps // 2
    core, my_x, my_y = info[0], info[1], info[2]

    if n_y:
        copies = []
        for i, piece in enumerate(pieces):
            c = core if i < n_y else 1 - core
            rows_of = weights.at[:, behind(my_y, i % n_y, n_y), c]
            copies.append(pltpu.make_async_copy(piece.at[:, :, pl.ds(first_lane, 2 * ch)], rows_of, sems.at[i]))
    else:
        copies = [pltpu.make_async_copy(pieces[0].at[:, pl.ds(first_lane, 2 * ch)], weights, sems.at[0])]
    for copy in copies:
        copy.start()
    if first is not None:
        first()

    def norm(first, step):
        here = pl.ds(first, step)
        squares = jnp.zeros((step, width), f32)
        for s in range(n_x):
            value = (streams[s][here] if n_s > 1 else streams[0][s, here]).astype(f32)
            squares += value * value
        mean = jnp.sum(squares, axis=-1, keepdims=True) * (1.0 / features)
        scale = lax.rsqrt(mean + norm_floor)
        for s in range(n_x):
            b = behind(my_x, s, n_x) if n_s > 1 else s
            wide = pl.ds(pl.multiple_of(b * width, width), width)
            value = (streams[s][here] if n_s > 1 else streams[0][s, here]).astype(f32)
            normed[here, wide] = (value * scale * gain[layer : layer + 1, wide]).astype(bf16)

    by_rows(rows, norm)
    for copy in copies:
        copy.wait()
    for half in range(2):
        part = weights[..., half * ch : (half + 1) * ch].reshape(features, ch)
        both[half] = jnp.dot(normed[...], part, preferred_element_type=f32)

    def gate(first, step):
        here = pl.ds(first, step)
        gated = both[0, here] * jax.nn.sigmoid(both[1, here])
        t = info[3 + layer] + first + lax.broadcasted_iota(jnp.int32, (step, 1), 0)
        gated = jnp.where((t >= 0) & (t < total), gated, 0.0).astype(bf16)
        padded[here] = gated.astype(f32)

    by_rows(rows, gate)
    columns[pl.ds(keep, 2 * ch - keep)] = jnp.zeros((2 * ch - keep, LANES), f32)

    def filtered(first, size):
        window = size + 2 * EDGE
        accs = []
        for start in range(0, ch, LANES):
            lanes = slice(start, start + LANES)
            win = padded[pl.ds(first, window), lanes]
            acc = jnp.zeros((size, LANES), f32) + bias[layer : layer + 1, lanes]
            for r in range(8):
                turned = pltpu.roll(win, window - r, 0) if r else win
                for q in range(window // 8):
                    k = 8 * q + r - shift
                    if 0 <= k < taps:
                        acc = acc + tap_ref[layer, k : k + 1, lanes] * turned[8 * q : 8 * q + size]
            accs.append(acc)
        mean = jnp.sum(sum(accs), axis=-1, keepdims=True) * (1.0 / ch)
        for start, acc in zip(range(0, ch, LANES), accs):
            for to in outs:
                to[pl.ds(first, size), start : start + LANES] = (acc - mean).astype(bf16)
        high = mean.astype(bf16).astype(f32)
        lane = lax.broadcasted_iota(jnp.int32, (size, LANES), 1)
        columns[pl.ds(first, size)] = jnp.where(lane == 0, high, jnp.where(lane == 1, mean - high, 0.0))

    by_rows(keep, filtered)
    across = columns[...].T[:8]
    params = jnp.concatenate([ln_gain[layer : layer + 1, :], ln_shift[layer : layer + 1, :]], axis=1)
    row = lax.broadcasted_iota(jnp.int32, across.shape, 0)
    for p in range(3):
        part = params.astype(bf16).astype(f32)
        across = jnp.where(row == 2 + p, part, across)
        params = params - part
    tail = jnp.concatenate([across[:, :ch], across[:, ch:]], axis=0).astype(bf16)
    for to in outs:
        to[keep:] = tail


def down_work(last, n_y, n_x, first_lane, info, exchanged, streams, pieces, out, weights, act, columns, sems):
    core, my_x, my_y = info[0], info[1], info[2]
    n_s = len(streams)
    gated = [exchanged.at[behind(my_x, s, n_x)] for s in range(n_x)]
    rows, ch = gated[0].shape
    keep = rows - EDGE
    width = out.shape[-1]

    copies = []

    def fetch(source, to):
        copies.append(pltpu.make_async_copy(source, to, sems.at[len(copies)]))

    if n_y:
        for i, piece in enumerate(pieces):
            c = core if i < n_y else 1 - core
            fetch(piece, weights.at[:, behind(my_y, i % n_y, n_y), c])
    elif last:
        mine = pl.ds(pl.multiple_of(my_x * width, width), width)
        fetch(pieces[0].at[mine, pl.ds(first_lane, n_x * ch)], weights)
    else:
        fetch(pieces[0].at[:, pl.ds(first_lane, n_x * ch)], weights)
    for copy in copies:
        copy.start()

    spans = []
    for s in range(n_x):
        tail = gated[s][keep:].astype(f32)
        spans.append(jnp.concatenate([tail[:8], tail[8:]], axis=1))
    params = [sum(v[2 + p : 3 + p] for p in range(3)) for v in spans]
    spans.append(jnp.zeros((LANES - 8 * n_x, 2 * ch), f32))
    columns[...] = jnp.concatenate(spans, axis=0).T

    def activate(first, size):
        here = pl.ds(first, size)
        cols = columns[here]
        means = [cols[:, 8 * s : 8 * s + 1] + cols[:, 8 * s + 1 : 8 * s + 2] for s in range(n_x)]
        average = sum(means) * (1.0 / n_x)
        squares = jnp.zeros((size, ch), f32)
        for s in range(n_x):
            value = gated[s][here].astype(f32) + (means[s] - average)
            squares += value * value
        mean = jnp.sum(squares, axis=-1, keepdims=True) * (1.0 / (n_x * ch))
        scale = lax.rsqrt(mean + norm_floor)
        for s in range(n_x):
            value = (gated[s][here].astype(f32) + (means[s] - average)) * scale
            value = value * params[s][:, :ch] + params[s][:, ch:]
            act[here, s * ch : (s + 1) * ch] = (value * jax.nn.sigmoid(value)).astype(bf16)

    by_rows(keep, activate)
    for copy in copies:
        copy.wait()
    dims = (((1,), (1,)), ((), ()))
    inner = slice(EDGE, EDGE + keep)
    if last:
        added = lax.dot_general(act[...], weights[...], dims, preferred_element_type=f32)
        out[...] = (streams[0][my_x, inner].astype(f32) + added).astype(bf16)
    else:
        part_rows = weights.shape[0] // n_x

        def block(b, base):
            part = weights[pl.ds(b * part_rows, part_rows)].reshape(width, n_x * ch)
            added = lax.dot_general(act[...], part, dims, preferred_element_type=f32)
            out[b] = (base.astype(f32) + added).astype(bf16)

        for s in range(n_x):
            if n_s > 1:
                block(behind(my_x, s, n_x), streams[s][inner])
            else:
                block(s, streams[0][s, inner])


def vmem():
    return pl.BlockSpec(memory_space=pltpu.VMEM)


def hbm():
    return pl.BlockSpec(memory_space=pltpu.HBM)


def smem():
    return pl.BlockSpec(memory_space=pltpu.SMEM)


def placed(pieces, features):
    if len(pieces) == 1:
        return 0, (features,)
    n_z, n_i, _ = pieces[0].shape
    return len(pieces) // 2, (n_z, len(pieces) // 2, 2, n_i)


def up_scratch(shape, rows, features, ch, n_y):
    return [
        pltpu.VMEM((*shape, 2 * ch), bf16),
        pltpu.VMEM((rows, features), bf16),
        pltpu.VMEM((2, rows, ch), f32),
        pltpu.VMEM((rows, ch), f32),
        pltpu.VMEM((2 * ch, LANES), f32),
        pltpu.SemaphoreType.DMA((max(1, 2 * n_y),)),
    ]


def down_scratch(shape, keep, n_x, ch, n_y):
    return [
        pltpu.VMEM((*shape, n_x * ch), bf16),
        pltpu.VMEM((keep, n_x * ch), bf16),
        pltpu.VMEM((2 * ch, LANES), f32),
        pltpu.SemaphoreType.DMA((max(1, 2 * n_y),)),
    ]


def up(layer, total, info, streams, params, pieces, ch, first_lane):
    rows, width = streams[0].shape[-2:]
    features = params[0].shape[1]
    n_y, shape = placed(pieces, features)
    return pl.pallas_call(
        functools.partial(up_kernel, layer, total, len(streams), n_y, first_lane),
        out_shape=jax.ShapeDtypeStruct((features // width, rows - EDGE, ch), bf16),
        in_specs=[smem()] + [vmem()] * (len(streams) + len(params)) + [hbm()] * len(pieces),
        out_specs=vmem(),
        scratch_shapes=up_scratch(shape, rows, features, ch, n_y),
    )(info, *streams, *params, *pieces)


def mid(layer, total, info, gated, streams, params, outs, down_lane, ups, up_lane):
    n_x, rows, ch = gated.shape
    keep = rows - EDGE
    width = streams[0].shape[-1]
    features = n_x * width
    n_out, out_shape = placed(outs, features)
    n_up, up_shape = placed(ups, features)
    return pl.pallas_call(
        functools.partial(mid_kernel, layer, total, len(streams), n_out, down_lane, n_up, up_lane, n_x),
        out_shape=(
            jax.ShapeDtypeStruct((n_x, keep, width), bf16),
            jax.ShapeDtypeStruct((n_x, keep - EDGE, ch), bf16),
        ),
        in_specs=[smem()] + [vmem()] * (1 + len(streams) + len(params)) + [hbm()] * (len(outs) + len(ups)),
        out_specs=(vmem(), vmem()),
        scratch_shapes=down_scratch(out_shape, keep, n_x, ch, n_out) + up_scratch(up_shape, keep, features, ch, n_up),
    )(info, gated, *streams, *params, *outs, *ups)


def down(info, gated, stream, piece, first_lane):
    n_x, rows, ch = gated.shape
    keep = rows - EDGE
    width = stream.shape[-1]
    return pl.pallas_call(
        functools.partial(down_kernel, n_x, first_lane),
        out_shape=jax.ShapeDtypeStruct((keep, width), bf16),
        in_specs=[smem()] + [vmem()] * 2 + [hbm()],
        out_specs=vmem(),
        scratch_shapes=down_scratch((width,), keep, n_x, ch, 0),
    )(info, gated, stream, piece)


def program(tokens, norm_gain, w_value, w_gate, conv_taps, conv_bias, ln_gain, ln_shift, w_out):
    layers, _, ch = w_value.shape
    n_x = lax.axis_size("x")
    my_x = lax.axis_index("x")
    n_tok, _ = tokens.shape
    halo = EDGE * layers
    size = lax.axis_size(SP)
    total = size * n_tok
    place = lax.axis_index(SP) * n_tok
    info = jnp.stack(
        [lax.axis_index("c"), my_x, lax.axis_index("y")]
        + [place - EDGE * (layers - l) for l in range(layers)]
    ).astype(jnp.int32)
    params = (norm_gain, conv_taps, conv_bias, ln_gain, ln_shift)

    def gather_z(array):
        return to_all(array, "z")

    near = min(2, layers)
    pairs = [w for l in range(near) for w in (w_value[l], w_gate[l])]
    ups = gather_z(jnp.concatenate(pairs, axis=1))

    wide = jnp.concatenate(spread(jnp.swapaxes(w_out, 1, 2), "x"), axis=-1)

    packs, lanes, at = [], [(0, 0)], 0
    for l in range(1, layers):
        pair = [w_value[l], w_gate[l]] if l >= near else []
        packs += [*pair, wide[l]]
        first = at if pair else 2 * ch * l
        lanes.append((first, at + 2 * ch * bool(pair)))
        at = lanes[-1][1] + n_x * ch
    rest = lax.all_gather(jnp.concatenate(packs, axis=1), SP, axis=0, tiled=True)

    before = lax.ppermute(tokens[n_tok - halo :], SP, [(i, i + 1) for i in range(size - 1)])
    following = lax.ppermute(tokens[:halo], SP, [(i + 1, i) for i in range(size - 1)])
    streams = spread(jnp.concatenate([before, tokens, following], axis=0), "x")

    ups = spread(ups, "y")
    outs = spread(gather_z(wide[0]), "y")
    ups = [*ups, *swap(ups)]
    near_out = swap(outs[:1])

    gated = up(0, total, info, streams, params, ups, ch, 0)
    for l in range(layers):
        gated = lax.all_to_all(gated, "x", split_axis=0, concat_axis=0, tiled=True)
        pieces = [rest]
        if l == 0:
            pieces = after(outs[1:], gated)
            pieces = [outs[0], *pieces, *near_out, *swap(pieces)]
        if l == layers - 1:
            return down(info, gated, streams[0], rest, lanes[l][1])
        up_pieces = ups if l + 1 < near else [rest]
        stream, gated = mid(l, total, info, gated, streams, params, pieces, lanes[l][1], up_pieces, lanes[l + 1][0])
        streams = [stream]


def solution(mesh):
    torus = Mesh(mesh.devices.reshape(8, 4, 2, mesh.shape["tp"]), ("z", "y", "c", "x"))
    return jax.shard_map(
        program,
        mesh=torus,
        in_specs=(
            P(SP, "x"),
            P(),
            P(None, SP, "x"),
            P(None, SP, "x"),
            P(None, None, "x"),
            P(None, "x"),
            P(None, "x"),
            P(None, "x"),
            P(None, "x", SP),
        ),
        out_specs=P(SP, "x"),
        check_vma=False,
    )
```

```python
import functools

import jax
import jax.numpy as jnp
from jax import lax
from jax.experimental import pallas as pl
from jax.experimental.pallas import tpu as pltpu
from jax.sharding import Mesh
from jax.sharding import PartitionSpec as P


SP = ("z", "y", "c")
EDGE = 16
LANES = 128
norm_floor = 0.01
bf16, f32 = jnp.bfloat16, jnp.float32


def to_all(array, axis):
    copies = jnp.broadcast_to(array, (lax.axis_size(axis), *array.shape))
    return lax.all_to_all(copies, axis, split_axis=0, concat_axis=0, tiled=True)


def shifted(array, axis, s):
    n = lax.axis_size(axis)
    return lax.ppermute(array, axis, [(i, (i + s) % n) for i in range(n)])


def spread(array, axis):
    n = lax.axis_size(axis)
    pieces = {s: shifted(array, axis, s) for s in (n // 2, 1, n - 1)}
    return [array] + [pieces[s] for s in range(1, n)]


def swap(arrays):
    return [shifted(a, "c", 1) for a in arrays]


def after(arrays, *others):
    return lax.optimization_barrier((tuple(arrays), *others))[0]


def behind(position, s, n):
    return lax.rem(position + (n - s), n)


def by_rows(rows, work, step=64):
    def one(i, carry):
        work(pl.multiple_of(i * step, step), step)
        return carry

    lax.fori_loop(0, rows // step, one, 0)
    if rows % step:
        work(rows - rows % step, rows % step)


def up_kernel(layer, total, n_s, n_y, first_lane, info, *refs):
    streams, params, refs = refs[:n_s], refs[n_s : n_s + 5], refs[n_s + 5 :]
    pieces, refs = refs[:-7], refs[-7:]
    up_work(layer, total, n_y, first_lane, info, streams, params, pieces, *refs)


def mid_kernel(layer, total, n_s, n_out, down_lane, n_up, up_lane, n_x, info, *refs):
    gated, refs = refs[:n_x], refs[n_x:]
    streams, params, refs = refs[:n_s], refs[n_s : n_s + 5], refs[n_s + 5 :]
    split = max(1, 2 * n_out)
    down_pieces, up_pieces, refs = refs[:split], refs[split:-12], refs[-12:]
    stream, out, refs = refs[0], refs[1], refs[2:]
    down_scratch, up_scratch = refs[:4], refs[4:]

    def first():
        down_work(False, n_out, n_x, down_lane, info, gated, streams, down_pieces, stream, *down_scratch)

    up_work(layer + 1, total, n_up, up_lane, info, [stream], params, up_pieces, out, *up_scratch, first=first)


def down_kernel(n_x, first_lane, info, *refs):
    gated, (stream, piece, out, *scratch) = refs[:n_x], refs[n_x:]
    down_work(True, 0, n_x, first_lane, info, gated, [stream], [piece], out, *scratch)


def up_work(
    layer, total, n_y, first_lane, info, streams, params, pieces, out, weights, normed, both, padded, columns, sems, first=None
):
    gain, tap_ref, bias, ln_gain, ln_shift = params
    n_s = len(streams)
    rows, features = normed.shape
    width = streams[0].shape[-1]
    n_x = features // width
    keep = rows - 2 * EDGE
    ch = out.shape[-1]
    taps = tap_ref.shape[1]
    shift = EDGE - taps // 2
    core, my_x, my_y = info[0], info[1], info[2]

    if n_y:
        copies = []
        for i, piece in enumerate(pieces):
            c = core if i < n_y else 1 - core
            rows_of = weights.at[:, behind(my_y, i % n_y, n_y), c]
            copies.append(pltpu.make_async_copy(piece.at[:, :, pl.ds(first_lane, 2 * ch)], rows_of, sems.at[i]))
    else:
        copies = [pltpu.make_async_copy(pieces[0].at[:, pl.ds(first_lane, 2 * ch)], weights, sems.at[0])]
    for copy in copies:
        copy.start()
    if first is not None:
        first()

    def norm(first, step):
        here = pl.ds(first, step)
        squares = jnp.zeros((step, width), f32)
        for s in range(n_x):
            value = (streams[s][here] if n_s > 1 else streams[0][s, here]).astype(f32)
            squares += value * value
        mean = jnp.sum(squares, axis=-1, keepdims=True) * (1.0 / features)
        scale = lax.rsqrt(mean + norm_floor)
        for s in range(n_x):
            b = behind(my_x, s, n_x) if n_s > 1 else s
            wide = pl.ds(pl.multiple_of(b * width, width), width)
            value = (streams[s][here] if n_s > 1 else streams[0][s, here]).astype(f32)
            normed[here, wide] = (value * scale * gain[layer : layer + 1, wide]).astype(bf16)

    by_rows(rows, norm)
    for copy in copies:
        copy.wait()
    for half in range(2):
        part = weights[..., half * ch : (half + 1) * ch].reshape(features, ch)
        both[half] = jnp.dot(normed[...], part, preferred_element_type=f32)

    def gate(first, step):
        here = pl.ds(first, step)
        gated = both[0, here] * jax.nn.sigmoid(both[1, here])
        t = info[3 + layer] + first + lax.broadcasted_iota(jnp.int32, (step, 1), 0)
        gated = jnp.where((t >= 0) & (t < total), gated, 0.0).astype(bf16)
        padded[here] = gated.astype(f32)

    by_rows(rows, gate)
    columns[pl.ds(keep, 2 * ch - keep)] = jnp.zeros((2 * ch - keep, LANES), f32)

    def filtered(first, size):
        window = size + 2 * EDGE
        accs = []
        for start in range(0, ch, LANES):
            lanes = slice(start, start + LANES)
            win = padded[pl.ds(first, window), lanes]
            acc = jnp.zeros((size, LANES), f32) + bias[layer : layer + 1, lanes]
            for r in range(8):
                turned = pltpu.roll(win, window - r, 0) if r else win
                for q in range(window // 8):
                    k = 8 * q + r - shift
                    if 0 <= k < taps:
                        acc = acc + tap_ref[layer, k : k + 1, lanes] * turned[8 * q : 8 * q + size]
            accs.append(acc)
        mean = jnp.sum(sum(accs), axis=-1, keepdims=True) * (1.0 / ch)
        for start, acc in zip(range(0, ch, LANES), accs):
            out[pl.ds(first, size), start : start + LANES] = (acc - mean).astype(bf16)
        high = mean.astype(bf16).astype(f32)
        lane = lax.broadcasted_iota(jnp.int32, (size, LANES), 1)
        columns[pl.ds(first, size)] = jnp.where(lane == 0, high, jnp.where(lane == 1, mean - high, 0.0))

    by_rows(keep, filtered)
    across = columns[...].T[:8]
    params = jnp.concatenate([ln_gain[layer : layer + 1, :], ln_shift[layer : layer + 1, :]], axis=1)
    row = lax.broadcasted_iota(jnp.int32, across.shape, 0)
    for p in range(3):
        part = params.astype(bf16).astype(f32)
        across = jnp.where(row == 2 + p, part, across)
        params = params - part
    tail = jnp.concatenate([across[:, :ch], across[:, ch:]], axis=0).astype(bf16)
    out[keep:] = tail


def down_work(last, n_y, n_x, first_lane, info, gated, streams, pieces, out, weights, act, columns, sems):
    core, my_x, my_y = info[0], info[1], info[2]
    n_s = len(streams)
    rows, ch = gated[0].shape
    keep = rows - EDGE
    width = out.shape[-1]

    copies = []

    def fetch(source, to):
        copies.append(pltpu.make_async_copy(source, to, sems.at[len(copies)]))

    if n_y:
        for i, piece in enumerate(pieces):
            c = core if i < n_y else 1 - core
            fetch(piece, weights.at[:, behind(my_y, i % n_y, n_y), c])
    elif last:
        mine = pl.ds(pl.multiple_of(my_x * width, width), width)
        fetch(pieces[0].at[mine, pl.ds(first_lane, n_x * ch)], weights)
    else:
        fetch(pieces[0].at[:, pl.ds(first_lane, n_x * ch)], weights)
    for copy in copies:
        copy.start()

    spans = []
    for s in range(n_x):
        tail = gated[s][keep:].astype(f32)
        spans.append(jnp.concatenate([tail[:8], tail[8:]], axis=1))
    params = [sum(v[2 + p : 3 + p] for p in range(3)) for v in spans]
    spans.append(jnp.zeros((LANES - 8 * n_x, 2 * ch), f32))
    columns[...] = jnp.concatenate(spans, axis=0).T

    def activate(first, size):
        here = pl.ds(first, size)
        cols = columns[here]
        means = [cols[:, 8 * s : 8 * s + 1] + cols[:, 8 * s + 1 : 8 * s + 2] for s in range(n_x)]
        average = sum(means) * (1.0 / n_x)
        squares = jnp.zeros((size, ch), f32)
        for s in range(n_x):
            value = gated[s][here].astype(f32) + (means[s] - average)
            squares += value * value
        mean = jnp.sum(squares, axis=-1, keepdims=True) * (1.0 / (n_x * ch))
        scale = lax.rsqrt(mean + norm_floor)
        for s in range(n_x):
            value = (gated[s][here].astype(f32) + (means[s] - average)) * scale
            value = value * params[s][:, :ch] + params[s][:, ch:]
            act[here, s * ch : (s + 1) * ch] = (value * jax.nn.sigmoid(value)).astype(bf16)

    by_rows(keep, activate)
    for copy in copies:
        copy.wait()
    dims = (((1,), (1,)), ((), ()))
    inner = slice(EDGE, EDGE + keep)
    if last:
        added = lax.dot_general(act[...], weights[...], dims, preferred_element_type=f32)
        out[...] = (streams[0][my_x, inner].astype(f32) + added).astype(bf16)
    else:
        part_rows = weights.shape[0] // n_x

        def block(b, base):
            part = weights[pl.ds(b * part_rows, part_rows)].reshape(width, n_x * ch)
            added = lax.dot_general(act[...], part, dims, preferred_element_type=f32)
            out[b] = (base.astype(f32) + added).astype(bf16)

        for s in range(n_x):
            if n_s > 1:
                block(behind(my_x, s, n_x), streams[s][inner])
            else:
                block(s, streams[0][s, inner])


def vmem():
    return pl.BlockSpec(memory_space=pltpu.VMEM)


def hbm():
    return pl.BlockSpec(memory_space=pltpu.HBM)


def smem():
    return pl.BlockSpec(memory_space=pltpu.SMEM)


def placed(pieces, features):
    if len(pieces) == 1:
        return 0, (features,)
    n_z, n_i, _ = pieces[0].shape
    return len(pieces) // 2, (n_z, len(pieces) // 2, 2, n_i)


def up_scratch(shape, rows, features, ch, n_y):
    return [
        pltpu.VMEM((*shape, 2 * ch), bf16),
        pltpu.VMEM((rows, features), bf16),
        pltpu.VMEM((2, rows, ch), f32),
        pltpu.VMEM((rows, ch), f32),
        pltpu.VMEM((2 * ch, LANES), f32),
        pltpu.SemaphoreType.DMA((max(1, 2 * n_y),)),
    ]


def down_scratch(shape, keep, n_x, ch, n_y):
    return [
        pltpu.VMEM((*shape, n_x * ch), bf16),
        pltpu.VMEM((keep, n_x * ch), bf16),
        pltpu.VMEM((2 * ch, LANES), f32),
        pltpu.SemaphoreType.DMA((max(1, 2 * n_y),)),
    ]


def up(layer, total, info, streams, params, pieces, ch, first_lane):
    rows = streams[0].shape[-2]
    features = params[0].shape[1]
    n_y, shape = placed(pieces, features)
    return pl.pallas_call(
        functools.partial(up_kernel, layer, total, len(streams), n_y, first_lane),
        out_shape=jax.ShapeDtypeStruct((rows - EDGE, ch), bf16),
        in_specs=[smem()] + [vmem()] * (len(streams) + len(params)) + [hbm()] * len(pieces),
        out_specs=vmem(),
        scratch_shapes=up_scratch(shape, rows, features, ch, n_y),
    )(info, *streams, *params, *pieces)


def mid(layer, total, info, gated, streams, params, outs, down_lane, ups, up_lane):
    n_x = len(gated)
    rows, ch = gated[0].shape
    keep = rows - EDGE
    width = streams[0].shape[-1]
    features = n_x * width
    n_out, out_shape = placed(outs, features)
    n_up, up_shape = placed(ups, features)
    return pl.pallas_call(
        functools.partial(mid_kernel, layer, total, len(streams), n_out, down_lane, n_up, up_lane, n_x),
        out_shape=(
            jax.ShapeDtypeStruct((n_x, keep, width), bf16),
            jax.ShapeDtypeStruct((keep - EDGE, ch), bf16),
        ),
        in_specs=[smem()] + [vmem()] * (n_x + len(streams) + len(params)) + [hbm()] * (len(outs) + len(ups)),
        out_specs=(vmem(), vmem()),
        scratch_shapes=down_scratch(out_shape, keep, n_x, ch, n_out) + up_scratch(up_shape, keep, features, ch, n_up),
    )(info, *gated, *streams, *params, *outs, *ups)


def down(info, gated, stream, piece, first_lane):
    n_x = len(gated)
    rows, ch = gated[0].shape
    keep = rows - EDGE
    width = stream.shape[-1]
    return pl.pallas_call(
        functools.partial(down_kernel, n_x, first_lane),
        out_shape=jax.ShapeDtypeStruct((keep, width), bf16),
        in_specs=[smem()] + [vmem()] * (n_x + 1) + [hbm()],
        out_specs=vmem(),
        scratch_shapes=down_scratch((width,), keep, n_x, ch, 0),
    )(info, *gated, stream, piece)


def program(tokens, norm_gain, w_value, w_gate, conv_taps, conv_bias, ln_gain, ln_shift, w_out):
    layers, _, ch = w_value.shape
    n_x = lax.axis_size("x")
    my_x = lax.axis_index("x")
    n_tok, _ = tokens.shape
    halo = EDGE * layers
    size = lax.axis_size(SP)
    total = size * n_tok
    place = lax.axis_index(SP) * n_tok
    info = jnp.stack(
        [lax.axis_index("c"), my_x, lax.axis_index("y")]
        + [place - EDGE * (layers - l) for l in range(layers)]
    ).astype(jnp.int32)
    params = (norm_gain, conv_taps, conv_bias, ln_gain, ln_shift)

    def gather_z(array):
        return to_all(array, "z")

    near = min(2, layers)
    pairs = [w for l in range(near) for w in (w_value[l], w_gate[l])]
    ups = gather_z(jnp.concatenate(pairs, axis=1))

    wide = jnp.concatenate(spread(jnp.swapaxes(w_out, 1, 2), "x"), axis=-1)

    packs, lanes, at = [], [(0, 0)], 0
    for l in range(1, layers):
        pair = [w_value[l], w_gate[l]] if l >= near else []
        packs += [*pair, wide[l]]
        first = at if pair else 2 * ch * l
        lanes.append((first, at + 2 * ch * bool(pair)))
        at = lanes[-1][1] + n_x * ch
    rest = lax.all_gather(jnp.concatenate(packs, axis=1), SP, axis=0, tiled=True)

    before = lax.ppermute(tokens[n_tok - halo :], SP, [(i, i + 1) for i in range(size - 1)])
    following = lax.ppermute(tokens[:halo], SP, [(i + 1, i) for i in range(size - 1)])
    streams = spread(jnp.concatenate([before, tokens, following], axis=0), "x")

    ups = spread(ups, "y")
    outs = spread(gather_z(wide[0]), "y")
    ups = [*ups, *swap(ups)]
    near_out = swap(outs[:1])

    gated = up(0, total, info, streams, params, ups, ch, 0)
    for l in range(layers):
        block, gated = gated, spread(gated, "x")
        pieces = [rest]
        if l == 0:
            pieces = after(outs[1:], block)
            pieces = [outs[0], *pieces, *near_out, *swap(pieces)]
        if l == layers - 1:
            return down(info, gated, streams[0], rest, lanes[l][1])
        up_pieces = ups if l + 1 < near else [rest]
        stream, gated = mid(l, total, info, gated, streams, params, pieces, lanes[l][1], up_pieces, lanes[l + 1][0])
        streams = [stream]


def solution(mesh):
    torus = Mesh(mesh.devices.reshape(8, 4, 2, mesh.shape["tp"]), ("z", "y", "c", "x"))
    return jax.shard_map(
        program,
        mesh=torus,
        in_specs=(
            P(SP, "x"),
            P(),
            P(None, SP, "x"),
            P(None, SP, "x"),
            P(None, None, "x"),
            P(None, "x"),
            P(None, "x"),
            P(None, "x"),
            P(None, "x", SP),
        ),
        out_specs=P(SP, "x"),
        check_vma=False,
    )
```

```python
import functools

import jax
import jax.numpy as jnp
from jax import lax
from jax.experimental import pallas as pl
from jax.experimental.pallas import tpu as pltpu
from jax.sharding import Mesh
from jax.sharding import PartitionSpec as P


SP = ("z", "y", "c")
EDGE = 16
LANES = 128
norm_floor = 0.01
bf16, f32 = jnp.bfloat16, jnp.float32


def to_all(array, axis):
    copies = jnp.broadcast_to(array, (lax.axis_size(axis), *array.shape))
    return lax.all_to_all(copies, axis, split_axis=0, concat_axis=0, tiled=True)


def shifted(array, axis, s):
    n = lax.axis_size(axis)
    return lax.ppermute(array, axis, [(i, (i + s) % n) for i in range(n)])


def spread(array, axis):
    n = lax.axis_size(axis)
    pieces = {s: shifted(array, axis, s) for s in (n // 2, 1, n - 1)}
    return [array] + [pieces[s] for s in range(1, n)]


def swap(arrays):
    return [shifted(a, "c", 1) for a in arrays]


def after(arrays, *others):
    return lax.optimization_barrier((tuple(arrays), *others))[0]


def behind(position, s, n):
    return lax.rem(position + (n - s), n)


def by_rows(rows, work, step=64):
    def one(i, carry):
        work(pl.multiple_of(i * step, step), step)
        return carry

    lax.fori_loop(0, rows // step, one, 0)
    if rows % step:
        work(rows - rows % step, rows % step)


def up_kernel(layer, total, n_s, n_y, first_lane, info, *refs):
    streams, params, refs = refs[:n_s], refs[n_s : n_s + 5], refs[n_s + 5 :]
    pieces, refs = refs[:-7], refs[-7:]
    up_work(layer, total, n_y, first_lane, info, streams, params, pieces, *refs)


def mid_kernel(layer, total, n_s, n_out, down_lane, n_up, up_lane, n_x, info, *refs):
    gated, refs = refs[:n_x], refs[n_x:]
    streams, params, refs = refs[:n_s], refs[n_s : n_s + 5], refs[n_s + 5 :]
    split = max(1, 2 * n_out)
    down_pieces, up_pieces, refs = refs[:split], refs[split:-12], refs[-12:]
    stream, out, refs = refs[0], refs[1], refs[2:]
    down_scratch, up_scratch = refs[:4], refs[4:]

    def first():
        down_work(False, n_out, n_x, down_lane, info, gated, streams, down_pieces, stream, *down_scratch)

    up_work(layer + 1, total, n_up, up_lane, info, [stream], params, up_pieces, out, *up_scratch, first=first)


def down_kernel(n_x, first_lane, info, *refs):
    gated, (stream, piece, out, *scratch) = refs[:n_x], refs[n_x:]
    down_work(True, 0, n_x, first_lane, info, gated, [stream], [piece], out, *scratch)


def up_work(
    layer, total, n_y, first_lane, info, streams, params, pieces, out, weights, normed, both, padded, columns, sems, first=None
):
    gain, tap_ref, bias, ln_gain, ln_shift = params
    n_s = len(streams)
    rows, features = normed.shape
    width = streams[0].shape[-1]
    n_x = features // width
    keep = rows - 2 * EDGE
    ch = out.shape[-1]
    taps = tap_ref.shape[1]
    shift = EDGE - taps // 2
    core, my_x, my_y = info[0], info[1], info[2]

    if n_y:
        copies = []
        for i, piece in enumerate(pieces):
            c = core if i < n_y else 1 - core
            rows_of = weights.at[:, behind(my_y, i % n_y, n_y), c]
            copies.append(pltpu.make_async_copy(piece.at[:, :, pl.ds(first_lane, 2 * ch)], rows_of, sems.at[i]))
    else:
        copies = [pltpu.make_async_copy(pieces[0].at[:, pl.ds(first_lane, 2 * ch)], weights, sems.at[0])]
    for copy in copies:
        copy.start()
    if first is not None:
        first()

    def norm(first, step):
        here = pl.ds(first, step)
        squares = jnp.zeros((step, width), f32)
        for s in range(n_x):
            value = (streams[s][here] if n_s > 1 else streams[0][s, here]).astype(f32)
            squares += value * value
        mean = jnp.sum(squares, axis=-1, keepdims=True) * (1.0 / features)
        scale = lax.rsqrt(mean + norm_floor)
        for s in range(n_x):
            b = behind(my_x, s, n_x) if n_s > 1 else s
            wide = pl.ds(pl.multiple_of(b * width, width), width)
            value = (streams[s][here] if n_s > 1 else streams[0][s, here]).astype(f32)
            normed[here, wide] = (value * scale * gain[layer : layer + 1, wide]).astype(bf16)

    by_rows(rows, norm, 128)
    for copy in copies:
        copy.wait()
    for half in range(2):
        part = weights[..., half * ch : (half + 1) * ch].reshape(features, ch)
        both[half] = jnp.dot(normed[...], part, preferred_element_type=f32)

    def gate(first, step):
        here = pl.ds(first, step)
        gated = both[0, here] * jax.nn.sigmoid(both[1, here])
        t = info[3 + layer] + first + lax.broadcasted_iota(jnp.int32, (step, 1), 0)
        gated = jnp.where((t >= 0) & (t < total), gated, 0.0).astype(bf16)
        padded[here] = gated.astype(f32)

    by_rows(rows, gate, 128)
    columns[pl.ds(keep, 2 * ch - keep)] = jnp.zeros((2 * ch - keep, LANES), f32)

    def filtered(first, size):
        window = size + 2 * EDGE
        accs = []
        for start in range(0, ch, LANES):
            lanes = slice(start, start + LANES)
            win = padded[pl.ds(first, window), lanes]
            acc = jnp.zeros((size, LANES), f32) + bias[layer : layer + 1, lanes]
            for r in range(8):
                turned = pltpu.roll(win, window - r, 0) if r else win
                for q in range(window // 8):
                    k = 8 * q + r - shift
                    if 0 <= k < taps:
                        acc = acc + tap_ref[layer, k : k + 1, lanes] * turned[8 * q : 8 * q + size]
            accs.append(acc)
        mean = jnp.sum(sum(accs), axis=-1, keepdims=True) * (1.0 / ch)
        for start, acc in zip(range(0, ch, LANES), accs):
            out[pl.ds(first, size), start : start + LANES] = (acc - mean).astype(bf16)
        high = mean.astype(bf16).astype(f32)
        lane = lax.broadcasted_iota(jnp.int32, (size, LANES), 1)
        columns[pl.ds(first, size)] = jnp.where(lane == 0, high, jnp.where(lane == 1, mean - high, 0.0))

    by_rows(keep, filtered)
    across = columns[...].T[:8]
    params = jnp.concatenate([ln_gain[layer : layer + 1, :], ln_shift[layer : layer + 1, :]], axis=1)
    row = lax.broadcasted_iota(jnp.int32, across.shape, 0)
    for p in range(3):
        part = params.astype(bf16).astype(f32)
        across = jnp.where(row == 2 + p, part, across)
        params = params - part
    tail = jnp.concatenate([across[:, :ch], across[:, ch:]], axis=0).astype(bf16)
    out[keep:] = tail


def down_work(last, n_y, n_x, first_lane, info, gated, streams, pieces, out, weights, act, columns, sems):
    core, my_x, my_y = info[0], info[1], info[2]
    n_s = len(streams)
    rows, ch = gated[0].shape
    keep = rows - EDGE
    width = out.shape[-1]

    copies = []

    def fetch(source, to):
        copies.append(pltpu.make_async_copy(source, to, sems.at[len(copies)]))

    if n_y:
        for i, piece in enumerate(pieces):
            c = core if i < n_y else 1 - core
            fetch(piece, weights.at[:, behind(my_y, i % n_y, n_y), c])
    elif last:
        mine = pl.ds(pl.multiple_of(my_x * width, width), width)
        fetch(pieces[0].at[mine, pl.ds(first_lane, n_x * ch)], weights)
    else:
        fetch(pieces[0].at[:, pl.ds(first_lane, n_x * ch)], weights)
    for copy in copies:
        copy.start()

    spans = []
    for s in range(n_x):
        tail = gated[s][keep:].astype(f32)
        spans.append(jnp.concatenate([tail[:8], tail[8:]], axis=1))
    params = [sum(v[2 + p : 3 + p] for p in range(3)) for v in spans]
    spans.append(jnp.zeros((LANES - 8 * n_x, 2 * ch), f32))
    columns[...] = jnp.concatenate(spans, axis=0).T

    def activate(first, size):
        here = pl.ds(first, size)
        cols = columns[here]
        means = [cols[:, 8 * s : 8 * s + 1] + cols[:, 8 * s + 1 : 8 * s + 2] for s in range(n_x)]
        average = sum(means) * (1.0 / n_x)
        squares = jnp.zeros((size, ch), f32)
        for s in range(n_x):
            value = gated[s][here].astype(f32) + (means[s] - average)
            squares += value * value
        mean = jnp.sum(squares, axis=-1, keepdims=True) * (1.0 / (n_x * ch))
        scale = lax.rsqrt(mean + norm_floor)
        for s in range(n_x):
            value = (gated[s][here].astype(f32) + (means[s] - average)) * scale
            value = value * params[s][:, :ch] + params[s][:, ch:]
            act[here, s * ch : (s + 1) * ch] = (value * jax.nn.sigmoid(value)).astype(bf16)

    by_rows(keep, activate, 128)
    for copy in copies:
        copy.wait()
    dims = (((1,), (1,)), ((), ()))
    inner = slice(EDGE, EDGE + keep)
    if last:
        added = lax.dot_general(act[...], weights[...], dims, preferred_element_type=f32)
        out[...] = (streams[0][my_x, inner].astype(f32) + added).astype(bf16)
    else:
        part_rows = weights.shape[0] // n_x

        def block(b, base):
            part = weights[pl.ds(b * part_rows, part_rows)].reshape(width, n_x * ch)
            added = lax.dot_general(act[...], part, dims, preferred_element_type=f32)
            out[b] = (base.astype(f32) + added).astype(bf16)

        for s in range(n_x):
            if n_s > 1:
                block(behind(my_x, s, n_x), streams[s][inner])
            else:
                block(s, streams[0][s, inner])


def vmem():
    return pl.BlockSpec(memory_space=pltpu.VMEM)


def hbm():
    return pl.BlockSpec(memory_space=pltpu.HBM)


def smem():
    return pl.BlockSpec(memory_space=pltpu.SMEM)


def placed(pieces, features):
    if len(pieces) == 1:
        return 0, (features,)
    n_z, n_i, _ = pieces[0].shape
    return len(pieces) // 2, (n_z, len(pieces) // 2, 2, n_i)


def up_scratch(shape, rows, features, ch, n_y):
    return [
        pltpu.VMEM((*shape, 2 * ch), bf16),
        pltpu.VMEM((rows, features), bf16),
        pltpu.VMEM((2, rows, ch), f32),
        pltpu.VMEM((rows, ch), f32),
        pltpu.VMEM((2 * ch, LANES), f32),
        pltpu.SemaphoreType.DMA((max(1, 2 * n_y),)),
    ]


def down_scratch(shape, keep, n_x, ch, n_y):
    return [
        pltpu.VMEM((*shape, n_x * ch), bf16),
        pltpu.VMEM((keep, n_x * ch), bf16),
        pltpu.VMEM((2 * ch, LANES), f32),
        pltpu.SemaphoreType.DMA((max(1, 2 * n_y),)),
    ]


def up(layer, total, info, streams, params, pieces, ch, first_lane):
    rows = streams[0].shape[-2]
    features = params[0].shape[1]
    n_y, shape = placed(pieces, features)
    return pl.pallas_call(
        functools.partial(up_kernel, layer, total, len(streams), n_y, first_lane),
        out_shape=jax.ShapeDtypeStruct((rows - EDGE, ch), bf16),
        in_specs=[smem()] + [vmem()] * (len(streams) + len(params)) + [hbm()] * len(pieces),
        out_specs=vmem(),
        scratch_shapes=up_scratch(shape, rows, features, ch, n_y),
    )(info, *streams, *params, *pieces)


def mid(layer, total, info, gated, streams, params, outs, down_lane, ups, up_lane):
    n_x = len(gated)
    rows, ch = gated[0].shape
    keep = rows - EDGE
    width = streams[0].shape[-1]
    features = n_x * width
    n_out, out_shape = placed(outs, features)
    n_up, up_shape = placed(ups, features)
    return pl.pallas_call(
        functools.partial(mid_kernel, layer, total, len(streams), n_out, down_lane, n_up, up_lane, n_x),
        out_shape=(
            jax.ShapeDtypeStruct((n_x, keep, width), bf16),
            jax.ShapeDtypeStruct((keep - EDGE, ch), bf16),
        ),
        in_specs=[smem()] + [vmem()] * (n_x + len(streams) + len(params)) + [hbm()] * (len(outs) + len(ups)),
        out_specs=(vmem(), vmem()),
        scratch_shapes=down_scratch(out_shape, keep, n_x, ch, n_out) + up_scratch(up_shape, keep, features, ch, n_up),
    )(info, *gated, *streams, *params, *outs, *ups)


def down(info, gated, stream, piece, first_lane):
    n_x = len(gated)
    rows, ch = gated[0].shape
    keep = rows - EDGE
    width = stream.shape[-1]
    return pl.pallas_call(
        functools.partial(down_kernel, n_x, first_lane),
        out_shape=jax.ShapeDtypeStruct((keep, width), bf16),
        in_specs=[smem()] + [vmem()] * (n_x + 1) + [hbm()],
        out_specs=vmem(),
        scratch_shapes=down_scratch((width,), keep, n_x, ch, 0),
    )(info, *gated, stream, piece)


def program(tokens, norm_gain, w_value, w_gate, conv_taps, conv_bias, ln_gain, ln_shift, w_out):
    layers, _, ch = w_value.shape
    n_x = lax.axis_size("x")
    my_x = lax.axis_index("x")
    n_tok, _ = tokens.shape
    halo = EDGE * layers
    size = lax.axis_size(SP)
    total = size * n_tok
    place = lax.axis_index(SP) * n_tok
    info = jnp.stack(
        [lax.axis_index("c"), my_x, lax.axis_index("y")]
        + [place - EDGE * (layers - l) for l in range(layers)]
    ).astype(jnp.int32)
    params = (norm_gain, conv_taps, conv_bias, ln_gain, ln_shift)

    def gather_z(array):
        return to_all(array, "z")

    near = min(2, layers)
    pairs = [w for l in range(near) for w in (w_value[l], w_gate[l])]
    ups = gather_z(jnp.concatenate(pairs, axis=1))

    wide = jnp.concatenate(spread(jnp.swapaxes(w_out, 1, 2), "x"), axis=-1)

    packs, lanes, at = [], [(0, 0)], 0
    for l in range(1, layers):
        pair = [w_value[l], w_gate[l]] if l >= near else []
        packs += [*pair, wide[l]]
        first = at if pair else 2 * ch * l
        lanes.append((first, at + 2 * ch * bool(pair)))
        at = lanes[-1][1] + n_x * ch
    rest = lax.all_gather(jnp.concatenate(packs, axis=1), SP, axis=0, tiled=True)

    before = lax.ppermute(tokens[n_tok - halo :], SP, [(i, i + 1) for i in range(size - 1)])
    following = lax.ppermute(tokens[:halo], SP, [(i + 1, i) for i in range(size - 1)])
    streams = spread(jnp.concatenate([before, tokens, following], axis=0), "x")

    ups = spread(ups, "y")
    outs = spread(gather_z(wide[0]), "y")
    ups = [*ups, *swap(ups)]
    near_out = swap(outs[:1])

    gated = up(0, total, info, streams, params, ups, ch, 0)
    for l in range(layers):
        block, gated = gated, spread(gated, "x")
        pieces = [rest]
        if l == 0:
            pieces = after(outs[1:], block)
            pieces = [outs[0], *pieces, *near_out, *swap(pieces)]
        if l == layers - 1:
            return down(info, gated, streams[0], rest, lanes[l][1])
        up_pieces = ups if l + 1 < near else [rest]
        stream, gated = mid(l, total, info, gated, streams, params, pieces, lanes[l][1], up_pieces, lanes[l + 1][0])
        streams = [stream]


def solution(mesh):
    torus = Mesh(mesh.devices.reshape(8, 4, 2, mesh.shape["tp"]), ("z", "y", "c", "x"))
    return jax.shard_map(
        program,
        mesh=torus,
        in_specs=(
            P(SP, "x"),
            P(),
            P(None, SP, "x"),
            P(None, SP, "x"),
            P(None, None, "x"),
            P(None, "x"),
            P(None, "x"),
            P(None, "x"),
            P(None, "x", SP),
        ),
        out_specs=P(SP, "x"),
        check_vma=False,
    )
```

```python
import functools

import jax
import jax.numpy as jnp
from jax import lax
from jax.experimental import pallas as pl
from jax.experimental.pallas import tpu as pltpu
from jax.sharding import Mesh
from jax.sharding import PartitionSpec as P


SP = ("z", "y", "c")
EDGE = 16
LANES = 128
norm_floor = 0.01
bf16, f32 = jnp.bfloat16, jnp.float32


def to_all(array, axis):
    copies = jnp.broadcast_to(array, (lax.axis_size(axis), *array.shape))
    return lax.all_to_all(copies, axis, split_axis=0, concat_axis=0, tiled=True)


def shifted(array, axis, s):
    n = lax.axis_size(axis)
    return lax.ppermute(array, axis, [(i, (i + s) % n) for i in range(n)])


def spread(array, axis):
    n = lax.axis_size(axis)
    pieces = {s: shifted(array, axis, s) for s in (n // 2, 1, n - 1)}
    return [array] + [pieces[s] for s in range(1, n)]


def swap(arrays):
    return [shifted(a, "c", 1) for a in arrays]


def after(arrays, *others):
    return lax.optimization_barrier((tuple(arrays), *others))[0]


def behind(position, s, n):
    return lax.rem(position + (n - s), n)


def by_rows(rows, work, step=64):
    def one(i, carry):
        work(pl.multiple_of(i * step, step), step)
        return carry

    lax.fori_loop(0, rows // step, one, 0)
    if rows % step:
        work(rows - rows % step, rows % step)


def up_kernel(layer, total, n_s, n_y, first_lane, info, *refs):
    streams, params, refs = refs[:n_s], refs[n_s : n_s + 5], refs[n_s + 5 :]
    pieces, refs = refs[:-7], refs[-7:]
    up_work(layer, total, n_y, first_lane, info, streams, params, pieces, *refs)


def mid_kernel(layer, total, n_s, n_out, down_lane, n_up, up_lane, n_x, info, *refs):
    gated, refs = refs[:n_x], refs[n_x:]
    streams, params, refs = refs[:n_s], refs[n_s : n_s + 5], refs[n_s + 5 :]
    split = max(1, 2 * n_out)
    down_pieces, up_pieces, refs = refs[:split], refs[split:-12], refs[-12:]
    stream, out, refs = refs[0], refs[1], refs[2:]
    down_scratch, up_scratch = refs[:4], refs[4:]

    def first():
        down_work(False, n_out, n_x, down_lane, info, gated, streams, down_pieces, stream, *down_scratch)

    up_work(layer + 1, total, n_up, up_lane, info, [stream], params, up_pieces, out, *up_scratch, first=first)


def down_kernel(n_x, first_lane, info, *refs):
    gated, (stream, piece, out, *scratch) = refs[:n_x], refs[n_x:]
    down_work(True, 0, n_x, first_lane, info, gated, [stream], [piece], out, *scratch)


def up_work(
    layer, total, n_y, first_lane, info, streams, params, pieces, out, weights, normed, both, padded, columns, sems, first=None
):
    gain, tap_ref, bias, ln_gain, ln_shift = params
    n_s = len(streams)
    rows, features = normed.shape
    width = streams[0].shape[-1]
    n_x = features // width
    keep = rows - 2 * EDGE
    ch = out.shape[-1]
    taps = tap_ref.shape[1]
    shift = EDGE - taps // 2
    core, my_x, my_y = info[0], info[1], info[2]

    if n_y:
        copies = []
        for i, piece in enumerate(pieces):
            c = core if i < n_y else 1 - core
            rows_of = weights.at[:, behind(my_y, i % n_y, n_y), c]
            copies.append(pltpu.make_async_copy(piece.at[:, :, pl.ds(first_lane, 2 * ch)], rows_of, sems.at[i]))
    else:
        copies = [pltpu.make_async_copy(pieces[0].at[:, pl.ds(first_lane, 2 * ch)], weights, sems.at[0])]
    for copy in copies:
        copy.start()
    if first is not None:
        first()

    def norm(first, step):
        here = pl.ds(first, step)
        squares = jnp.zeros((step, width), f32)
        for s in range(n_x):
            value = (streams[s][here] if n_s > 1 else streams[0][s, here]).astype(f32)
            squares += value * value
        mean = jnp.sum(squares, axis=-1, keepdims=True) * (1.0 / features)
        scale = lax.rsqrt(mean + norm_floor)
        for s in range(n_x):
            b = behind(my_x, s, n_x) if n_s > 1 else s
            wide = pl.ds(pl.multiple_of(b * width, width), width)
            value = (streams[s][here] if n_s > 1 else streams[0][s, here]).astype(f32)
            normed[here, wide] = (value * scale * gain[layer : layer + 1, wide]).astype(bf16)

    by_rows(rows, norm, rows // 2)
    for copy in copies:
        copy.wait()
    for half in range(2):
        part = weights[..., half * ch : (half + 1) * ch].reshape(features, ch)
        both[half] = jnp.dot(normed[...], part, preferred_element_type=f32)

    def gate(first, step):
        here = pl.ds(first, step)
        gated = both[0, here] * jax.nn.sigmoid(both[1, here])
        t = info[3 + layer] + first + lax.broadcasted_iota(jnp.int32, (step, 1), 0)
        gated = jnp.where((t >= 0) & (t < total), gated, 0.0).astype(bf16)
        padded[here] = gated.astype(f32)

    by_rows(rows, gate, rows // 2)
    columns[pl.ds(keep, 2 * ch - keep)] = jnp.zeros((2 * ch - keep, LANES), f32)

    def filtered(first, size):
        window = size + 2 * EDGE
        accs = []
        for start in range(0, ch, LANES):
            lanes = slice(start, start + LANES)
            win = padded[pl.ds(first, window), lanes]
            acc = jnp.zeros((size, LANES), f32) + bias[layer : layer + 1, lanes]
            for r in range(8):
                turned = pltpu.roll(win, window - r, 0) if r else win
                for q in range(window // 8):
                    k = 8 * q + r - shift
                    if 0 <= k < taps:
                        acc = acc + tap_ref[layer, k : k + 1, lanes] * turned[8 * q : 8 * q + size]
            accs.append(acc)
        mean = jnp.sum(sum(accs), axis=-1, keepdims=True) * (1.0 / ch)
        for start, acc in zip(range(0, ch, LANES), accs):
            out[pl.ds(first, size), start : start + LANES] = (acc - mean).astype(bf16)
        high = mean.astype(bf16).astype(f32)
        lane = lax.broadcasted_iota(jnp.int32, (size, LANES), 1)
        columns[pl.ds(first, size)] = jnp.where(lane == 0, high, jnp.where(lane == 1, mean - high, 0.0))

    by_rows(keep, filtered)
    across = columns[...].T[:8]
    params = jnp.concatenate([ln_gain[layer : layer + 1, :], ln_shift[layer : layer + 1, :]], axis=1)
    row = lax.broadcasted_iota(jnp.int32, across.shape, 0)
    for p in range(3):
        part = params.astype(bf16).astype(f32)
        across = jnp.where(row == 2 + p, part, across)
        params = params - part
    tail = jnp.concatenate([across[:, :ch], across[:, ch:]], axis=0).astype(bf16)
    out[keep:] = tail


def down_work(last, n_y, n_x, first_lane, info, gated, streams, pieces, out, weights, act, columns, sems):
    core, my_x, my_y = info[0], info[1], info[2]
    n_s = len(streams)
    rows, ch = gated[0].shape
    keep = rows - EDGE
    width = out.shape[-1]

    copies = []

    def fetch(source, to):
        copies.append(pltpu.make_async_copy(source, to, sems.at[len(copies)]))

    if n_y:
        for i, piece in enumerate(pieces):
            c = core if i < n_y else 1 - core
            fetch(piece, weights.at[:, behind(my_y, i % n_y, n_y), c])
    elif last:
        mine = pl.ds(pl.multiple_of(my_x * width, width), width)
        fetch(pieces[0].at[mine, pl.ds(first_lane, n_x * ch)], weights)
    else:
        fetch(pieces[0].at[:, pl.ds(first_lane, n_x * ch)], weights)
    for copy in copies:
        copy.start()

    spans = []
    for s in range(n_x):
        tail = gated[s][keep:].astype(f32)
        spans.append(jnp.concatenate([tail[:8], tail[8:]], axis=1))
    params = [sum(v[2 + p : 3 + p] for p in range(3)) for v in spans]
    spans.append(jnp.zeros((LANES - 8 * n_x, 2 * ch), f32))
    columns[...] = jnp.concatenate(spans, axis=0).T

    def activate(first, size):
        here = pl.ds(first, size)
        cols = columns[here]
        means = [cols[:, 8 * s : 8 * s + 1] + cols[:, 8 * s + 1 : 8 * s + 2] for s in range(n_x)]
        average = sum(means) * (1.0 / n_x)
        squares = jnp.zeros((size, ch), f32)
        for s in range(n_x):
            value = gated[s][here].astype(f32) + (means[s] - average)
            squares += value * value
        mean = jnp.sum(squares, axis=-1, keepdims=True) * (1.0 / (n_x * ch))
        scale = lax.rsqrt(mean + norm_floor)
        for s in range(n_x):
            value = (gated[s][here].astype(f32) + (means[s] - average)) * scale
            value = value * params[s][:, :ch] + params[s][:, ch:]
            act[here, s * ch : (s + 1) * ch] = (value * jax.nn.sigmoid(value)).astype(bf16)

    by_rows(keep, activate, keep // 2)
    for copy in copies:
        copy.wait()
    dims = (((1,), (1,)), ((), ()))
    inner = slice(EDGE, EDGE + keep)
    if last:
        added = lax.dot_general(act[...], weights[...], dims, preferred_element_type=f32)
        out[...] = (streams[0][my_x, inner].astype(f32) + added).astype(bf16)
    else:
        part_rows = weights.shape[0] // n_x

        def block(b, base):
            part = weights[pl.ds(b * part_rows, part_rows)].reshape(width, n_x * ch)
            added = lax.dot_general(act[...], part, dims, preferred_element_type=f32)
            out[b] = (base.astype(f32) + added).astype(bf16)

        for s in range(n_x):
            if n_s > 1:
                block(behind(my_x, s, n_x), streams[s][inner])
            else:
                block(s, streams[0][s, inner])


def vmem():
    return pl.BlockSpec(memory_space=pltpu.VMEM)


def hbm():
    return pl.BlockSpec(memory_space=pltpu.HBM)


def smem():
    return pl.BlockSpec(memory_space=pltpu.SMEM)


def placed(pieces, features):
    if len(pieces) == 1:
        return 0, (features,)
    n_z, n_i, _ = pieces[0].shape
    return len(pieces) // 2, (n_z, len(pieces) // 2, 2, n_i)


def up_scratch(shape, rows, features, ch, n_y):
    return [
        pltpu.VMEM((*shape, 2 * ch), bf16),
        pltpu.VMEM((rows, features), bf16),
        pltpu.VMEM((2, rows, ch), f32),
        pltpu.VMEM((rows, ch), f32),
        pltpu.VMEM((2 * ch, LANES), f32),
        pltpu.SemaphoreType.DMA((max(1, 2 * n_y),)),
    ]


def down_scratch(shape, keep, n_x, ch, n_y):
    return [
        pltpu.VMEM((*shape, n_x * ch), bf16),
        pltpu.VMEM((keep, n_x * ch), bf16),
        pltpu.VMEM((2 * ch, LANES), f32),
        pltpu.SemaphoreType.DMA((max(1, 2 * n_y),)),
    ]


def up(layer, total, info, streams, params, pieces, ch, first_lane):
    rows = streams[0].shape[-2]
    features = params[0].shape[1]
    n_y, shape = placed(pieces, features)
    return pl.pallas_call(
        functools.partial(up_kernel, layer, total, len(streams), n_y, first_lane),
        out_shape=jax.ShapeDtypeStruct((rows - EDGE, ch), bf16),
        in_specs=[smem()] + [vmem()] * (len(streams) + len(params)) + [hbm()] * len(pieces),
        out_specs=vmem(),
        scratch_shapes=up_scratch(shape, rows, features, ch, n_y),
    )(info, *streams, *params, *pieces)


def mid(layer, total, info, gated, streams, params, outs, down_lane, ups, up_lane):
    n_x = len(gated)
    rows, ch = gated[0].shape
    keep = rows - EDGE
    width = streams[0].shape[-1]
    features = n_x * width
    n_out, out_shape = placed(outs, features)
    n_up, up_shape = placed(ups, features)
    return pl.pallas_call(
        functools.partial(mid_kernel, layer, total, len(streams), n_out, down_lane, n_up, up_lane, n_x),
        out_shape=(
            jax.ShapeDtypeStruct((n_x, keep, width), bf16),
            jax.ShapeDtypeStruct((keep - EDGE, ch), bf16),
        ),
        in_specs=[smem()] + [vmem()] * (n_x + len(streams) + len(params)) + [hbm()] * (len(outs) + len(ups)),
        out_specs=(vmem(), vmem()),
        scratch_shapes=down_scratch(out_shape, keep, n_x, ch, n_out) + up_scratch(up_shape, keep, features, ch, n_up),
    )(info, *gated, *streams, *params, *outs, *ups)


def down(info, gated, stream, piece, first_lane):
    n_x = len(gated)
    rows, ch = gated[0].shape
    keep = rows - EDGE
    width = stream.shape[-1]
    return pl.pallas_call(
        functools.partial(down_kernel, n_x, first_lane),
        out_shape=jax.ShapeDtypeStruct((keep, width), bf16),
        in_specs=[smem()] + [vmem()] * (n_x + 1) + [hbm()],
        out_specs=vmem(),
        scratch_shapes=down_scratch((width,), keep, n_x, ch, 0),
    )(info, *gated, stream, piece)


def program(tokens, norm_gain, w_value, w_gate, conv_taps, conv_bias, ln_gain, ln_shift, w_out):
    layers, _, ch = w_value.shape
    n_x = lax.axis_size("x")
    my_x = lax.axis_index("x")
    n_tok, _ = tokens.shape
    halo = EDGE * layers
    size = lax.axis_size(SP)
    total = size * n_tok
    place = lax.axis_index(SP) * n_tok
    info = jnp.stack(
        [lax.axis_index("c"), my_x, lax.axis_index("y")]
        + [place - EDGE * (layers - l) for l in range(layers)]
    ).astype(jnp.int32)
    params = (norm_gain, conv_taps, conv_bias, ln_gain, ln_shift)

    def gather_z(array):
        return to_all(array, "z")

    near = min(2, layers)
    pairs = [w for l in range(near) for w in (w_value[l], w_gate[l])]
    ups = gather_z(jnp.concatenate(pairs, axis=1))

    wide = jnp.concatenate(spread(jnp.swapaxes(w_out, 1, 2), "x"), axis=-1)

    packs, lanes, at = [], [(0, 0)], 0
    for l in range(1, layers):
        pair = [w_value[l], w_gate[l]] if l >= near else []
        packs += [*pair, wide[l]]
        first = at if pair else 2 * ch * l
        lanes.append((first, at + 2 * ch * bool(pair)))
        at = lanes[-1][1] + n_x * ch
    rest = lax.all_gather(jnp.concatenate(packs, axis=1), SP, axis=0, tiled=True)

    before = lax.ppermute(tokens[n_tok - halo :], SP, [(i, i + 1) for i in range(size - 1)])
    following = lax.ppermute(tokens[:halo], SP, [(i + 1, i) for i in range(size - 1)])
    streams = spread(jnp.concatenate([before, tokens, following], axis=0), "x")

    ups = spread(ups, "y")
    outs = spread(gather_z(wide[0]), "y")
    ups = [*ups, *swap(ups)]
    near_out = swap(outs[:1])

    gated = up(0, total, info, streams, params, ups, ch, 0)
    for l in range(layers):
        block, gated = gated, spread(gated, "x")
        pieces = [rest]
        if l == 0:
            pieces = after(outs[1:], block)
            pieces = [outs[0], *pieces, *near_out, *swap(pieces)]
        if l == layers - 1:
            return down(info, gated, streams[0], rest, lanes[l][1])
        up_pieces = ups if l + 1 < near else [rest]
        stream, gated = mid(l, total, info, gated, streams, params, pieces, lanes[l][1], up_pieces, lanes[l + 1][0])
        streams = [stream]


def solution(mesh):
    torus = Mesh(mesh.devices.reshape(8, 4, 2, mesh.shape["tp"]), ("z", "y", "c", "x"))
    return jax.shard_map(
        program,
        mesh=torus,
        in_specs=(
            P(SP, "x"),
            P(),
            P(None, SP, "x"),
            P(None, SP, "x"),
            P(None, None, "x"),
            P(None, "x"),
            P(None, "x"),
            P(None, "x"),
            P(None, "x", SP),
        ),
        out_specs=P(SP, "x"),
        check_vma=False,
    )
```
